32 devices in a mesh: rep: 2 (over x), fs: 8 (over z, y), tp: 2 (over core).
Axes of the slice: x: 2, y: 2, z: 4, core: 2. Of those that a mesh axis runs over, the one named last changes fastest.
Arguments:
- tokens: bfloat16 [5120, 2048], P(('rep', 'fs'), 'tp'), may hold values from -30 to 30
- mixer_gain: float32 [2048], P('tp'), may hold values from 0.1 to 1.9
- outer_weight: float32 [2048, 1024], P('fs', 'tp'), may hold values from -0.125 to 0.125
- inner_weight: float32 [2048, 1024], P('fs', 'tp'), may hold values from -0.125 to 0.125
- value_weight: float32 [2048, 1024], P('fs', 'tp'), may hold values from -0.125 to 0.125
- outer_scale: float32 [1024], P(('tp', 'fs')), may hold values from 0.5 to 2
- inner_scale: float32 [1024], P(('tp', 'fs')), may hold values from 0.5 to 2
- value_scale: float32 [1024], P(('tp', 'fs')), may hold values from 0.5 to 2
- mixer_taps: float32 [3, 1024], P(None, 'tp'), may hold values from -3.5 to 3.5
- mixer_project: float32 [1024, 2048], P('tp', 'fs'), may hold values from -0.1875 to 0.1875
- project_scale: float32 [2048], P('fs'), may hold values from 0.5 to 2
- channel_gain: float32 [2048], P('tp'), may hold values from 0.1 to 1.9
- gate_weight: float32 [2048, 5632], P('fs', 'tp'), may hold values from -0.125 to 0.125
- gate_scale: float32 [5632], P(('tp', 'fs')), may hold values from 0.5 to 2
- up_weight: float32 [2048, 5632], P('fs', 'tp'), may hold values from -0.125 to 0.125
- up_scale: float32 [5632], P(('tp', 'fs')), may hold values from 0.5 to 2
- channel_taps: float32 [3, 5632], P(None, 'tp'), may hold values from -3.5 to 3.5
- channel_bias: float32 [5632], P('tp'), may hold values from -3 to 3
- down_weight: float32 [5632, 2048], P('tp', 'fs'), may hold values from -0.078125 to 0.078125
- down_scale: float32 [2048], P('fs'), may hold values from 0.5 to 2
Outputs:
- result: bfloat16 [5120, 2048], P(('rep', 'fs'), 'tp')
The draws below stay inside these ranges and needn't reach their ends.
All inputs are finite; a program needn't handle non-finite values.
Results may differ from the reference program's by a relative error of at most 0.015.
Values may be sent and summed in bfloat16 or wider, within the bound.
A program may use at most 128 MiB of HBM per device.

```python
import math
import jax
import jax.numpy as jnp
from jax import lax

D = 2048
CW = 1024
FF = 5632
TAPS = 3
LEN = 320
TOKENS = 5120
N_TP = 2


def draw_tokens(key, part):
    first_key, second_key, third_key = jax.random.split(jax.random.fold_in(key, 11), 3)
    rough = jnp.exp(jax.random.uniform(second_key, (D,), jnp.float32, -0.7, 0.7))
    row_scale = jnp.exp(jax.random.uniform(third_key, (TOKENS, 1), jnp.float32, math.log(0.3), math.log(3.0)))
    rising = jnp.exp(jnp.linspace(0.0, math.log(3.0), D)).astype(jnp.float32)
    values = jax.random.normal(first_key, (TOKENS, D), jnp.float32) * row_scale * rough * rising
    return jnp.clip(values, -30.0, 30.0).astype(jnp.bfloat16)


def block_levels(stream_key, extent, cuts, smallest, top_value):
    level, own = 1.0, jax.random.fold_in(stream_key, 6)
    for axis_at, blocks in cuts:
        draws = jnp.exp(jax.random.uniform(jax.random.fold_in(own, axis_at), (blocks,), jnp.float32, smallest / len(cuts), top_value / len(cuts)))
        level = level * jnp.repeat(draws, extent[axis_at] // blocks).reshape([-1 if axis == axis_at else 1 for axis in range(len(extent))])
    return level


def centred(stream_key, extent, spread, most, cuts=(), held_as=jnp.bfloat16):
    result = spread * jax.random.normal(stream_key, extent, jnp.float32)
    if cuts:
        result = result * block_levels(stream_key, extent, cuts, -0.22, 0.18)
    return jnp.clip(result, -most, most).astype(held_as)


def setup_inputs(seed: int = 0) -> dict:
    arg_keys = jax.random.split(jax.random.key(seed), 21)
    return {
        "tokens": draw_tokens(jax.random.fold_in(arg_keys[20], 71), 0),
        "mixer_gain": jnp.clip(1.0 + 0.18 * jax.random.normal(arg_keys[1], (D,), jnp.float32), 0.1, 1.9),
        "outer_weight": centred(arg_keys[2], (D, CW), D ** -0.5, 0.125, ((0, 8), (1, 2)), jnp.float32),
        "inner_weight": centred(arg_keys[3], (D, CW), D ** -0.5, 0.125, ((0, 8), (1, 2)), jnp.float32),
        "value_weight": centred(arg_keys[4], (D, CW), D ** -0.5, 0.125, ((0, 8), (1, 2)), jnp.float32),
        "outer_scale": jnp.clip(jnp.exp(math.log(2.0) - 1.3862944 * jax.random.uniform(arg_keys[5], (CW,), jnp.float32) ** block_levels(arg_keys[5], (CW,), ((0, 16),), -0.2, 0.2)), 0.5, 2.0),
        "inner_scale": jnp.clip(jnp.exp(math.log(2.0) - 1.3862944 * jax.random.uniform(arg_keys[6], (CW,), jnp.float32) ** block_levels(arg_keys[6], (CW,), ((0, 16),), -0.2, 0.2)), 0.5, 2.0),
        "value_scale": jnp.clip(jnp.exp(math.log(2.0) - 1.3862944 * jax.random.uniform(arg_keys[7], (CW,), jnp.float32) ** block_levels(arg_keys[7], (CW,), ((0, 16),), -0.2, 0.2)), 0.5, 2.0),
        "mixer_taps": centred(arg_keys[8], (TAPS, CW), TAPS ** -0.5, 3.5, ((1, 2),), jnp.float32),
        "mixer_project": centred(arg_keys[9], (CW, D), CW ** -0.5, 0.1875, ((0, 2), (1, 8)), jnp.float32),
        "project_scale": jnp.clip(jnp.exp(math.log(2.0) - 1.3862944 * jax.random.uniform(arg_keys[10], (D,), jnp.float32) ** block_levels(arg_keys[10], (D,), ((0, 8),), -0.2, 0.2)), 0.5, 2.0),
        "channel_gain": jnp.clip(1.0 + 0.18 * jax.random.normal(arg_keys[11], (D,), jnp.float32), 0.1, 1.9),
        "gate_weight": centred(arg_keys[12], (D, FF), D ** -0.5, 0.125, ((0, 8), (1, 2)), jnp.float32),
        "gate_scale": jnp.clip(jnp.exp(math.log(2.0) - 1.3862944 * jax.random.uniform(arg_keys[13], (FF,), jnp.float32) ** block_levels(arg_keys[13], (FF,), ((0, 16),), -0.2, 0.2)), 0.5, 2.0),
        "up_weight": centred(arg_keys[14], (D, FF), D ** -0.5, 0.125, ((0, 8), (1, 2)), jnp.float32),
        "up_scale": jnp.clip(jnp.exp(math.log(2.0) - 1.3862944 * jax.random.uniform(arg_keys[15], (FF,), jnp.float32) ** block_levels(arg_keys[15], (FF,), ((0, 16),), -0.2, 0.2)), 0.5, 2.0),
        "channel_taps": centred(arg_keys[16], (TAPS, FF), TAPS ** -0.5, 3.5, ((1, 2),), jnp.float32),
        "channel_bias": centred(arg_keys[17], (FF,), 0.5, 3.0, ((0, 2),), jnp.float32),
        "down_weight": centred(arg_keys[18], (FF, D), FF ** -0.5, 0.078125, ((0, 2), (1, 8)), jnp.float32),
        "down_scale": jnp.clip(jnp.exp(math.log(2.0) - 1.3862944 * jax.random.uniform(arg_keys[19], (D,), jnp.float32) ** block_levels(arg_keys[19], (D,), ((0, 8),), -0.2, 0.2)), 0.5, 2.0),
    }


epsilon = 1e-06

def normalize(token_rows, gain):
    values = token_rows.astype(jnp.float32)
    inverse = lax.rsqrt(lax.optimization_barrier(jnp.sum(values * values, axis=1, keepdims=True)) / values.shape[1] + epsilon)
    return (values * inverse * gain.astype(jnp.float32)).astype(jnp.bfloat16)

def causal_taps(values, taps):
    tap_count = taps.shape[0]
    length = values.shape[0]
    padded = jnp.pad(values, ((tap_count - 1, 0), (0, 0)))
    running = jnp.zeros_like(values)
    for offset in range(tap_count):
        running = running + taps[offset].astype(jnp.float32) * padded[offset:offset + length]
    return running

def block_sums(hidden, weight, scale, blocks):
    length, channels = hidden.shape
    pieces = hidden.reshape(length, blocks, channels // blocks).astype(jnp.float32)
    matrices = weight.reshape(blocks, channels // blocks, weight.shape[1]).astype(jnp.float32)
    partials = jnp.einsum('lbc,bcd->bld', pieces, matrices) * scale.astype(jnp.float32)
    rounded = lax.optimization_barrier(partials.astype(jnp.bfloat16))
    return lax.optimization_barrier(jnp.sum(rounded.astype(jnp.float32), axis=0))

def scaled_product(normed, weight, scale):
    return jnp.dot(normed, weight, preferred_element_type=jnp.float32) * scale.astype(jnp.float32)

def reference(tokens, mixer_gain, outer_weight, inner_weight, value_weight, outer_scale, inner_scale, value_scale, mixer_taps, mixer_project, project_scale, channel_gain, gate_weight, gate_scale, up_weight, up_scale, channel_taps, channel_bias, down_weight, down_scale):
    outer_low = outer_weight.astype(jnp.bfloat16)
    inner_low = inner_weight.astype(jnp.bfloat16)
    value_low = value_weight.astype(jnp.bfloat16)
    project_low = mixer_project.astype(jnp.bfloat16)
    gate_low = gate_weight.astype(jnp.bfloat16)
    up_low = up_weight.astype(jnp.bfloat16)
    down_low = down_weight.astype(jnp.bfloat16)

    def one_sequence(token_rows):
        normed = normalize(token_rows, mixer_gain)
        outer_part = scaled_product(normed, outer_low, outer_scale)
        inner_part = scaled_product(normed, inner_low, inner_scale)
        value_part = scaled_product(normed, value_low, value_scale)
        mixed = (outer_part * causal_taps(inner_part * value_part, mixer_taps)).astype(jnp.bfloat16)
        middle = (token_rows.astype(jnp.float32) + block_sums(mixed, project_low, project_scale, N_TP)).astype(jnp.bfloat16)
        normed_two = normalize(middle, channel_gain)
        gate_part = scaled_product(normed_two, gate_low, gate_scale)
        up_part = scaled_product(normed_two, up_low, up_scale)
        hidden = (jax.nn.silu(causal_taps(gate_part, channel_taps) + channel_bias.astype(jnp.float32)) * up_part).astype(jnp.bfloat16)
        return (middle.astype(jnp.float32) + block_sums(hidden, down_low, down_scale, N_TP)).astype(jnp.bfloat16)
    sequences = tokens.reshape(tokens.shape[0] // LEN, LEN, tokens.shape[1])
    return lax.map(one_sequence, sequences).reshape(tokens.shape)
```

```python
import functools

import jax
import jax.numpy as jnp
from jax import lax
from jax.experimental import pallas as pl
from jax.experimental.pallas import tpu as pltpu
from jax.sharding import PartitionSpec as P

LEN = 320
GROUPS = 4
LANES = 128
SEMAPHORES = 256
VMEM_BYTES = 65000 * 1024
MESH = pl.DeviceIdType.MESH

epsilon = 1e-06
low = jnp.bfloat16


class Place:
    def __init__(self):
        self.fs = lax.axis_size("fs")
        self.reps = lax.axis_size("rep")
        self.tps = lax.axis_size("tp")
        self.slow = GROUPS if self.fs % GROUPS == 0 else 1
        self.fast = self.fs // self.slow
        at = lax.axis_index("fs")
        self.z, self.y = at // self.fast, at % self.fast
        self.r, self.t = lax.axis_index("rep"), lax.axis_index("tp")

    def from_slow(self, block, shift):
        perm = [(z * self.fast + y, (z - shift) % self.slow * self.fast + y)
                for z in range(self.slow) for y in range(self.fast)]
        return lax.ppermute(block, "fs", perm)

    def from_fast(self, block, shift):
        perm = [(z * self.fast + y, z * self.fast + (y - shift) % self.fast)
                for z in range(self.slow) for y in range(self.fast)]
        return lax.ppermute(block, "fs", perm)

    def from_rep(self, block, shift):
        return lax.ppermute(block, "rep", [(i, (i - shift) % self.reps) for i in range(self.reps)])

    def from_tp(self, block, shift):
        return lax.ppermute(block, "tp", [(i, (i - shift) % self.tps) for i in range(self.tps)])

    def spread(self, pieces, axis):
        held = jnp.concatenate(pieces, axis)
        held = jnp.concatenate([held] + [self.from_fast(held, j) for j in range(1, self.fast)], axis)
        return jnp.concatenate([held] + [self.from_rep(held, i) for i in range(1, self.reps)], axis)

    def order(self, width):
        return [
            (((self.z + k) % self.slow * self.fast + (self.y + j) % self.fast) * self.reps
             + (self.r + i) % self.reps) * width
            for i in range(self.reps) for j in range(self.fast) for k in range(self.slow)
        ]

    def position(self, block):
        f, part = block // self.reps, block % self.reps
        i = (part - self.r) % self.reps
        j = (f % self.fast - self.y) % self.fast
        k = (f // self.fast - self.z) % self.slow
        return (i * self.fast + j) * self.slow + k


def columns(values, offsets, width):
    return jnp.concatenate(
        [lax.dynamic_slice(values, (0, offset), (values.shape[0], width)) for offset in offsets], axis=1
    )


def inverse_norm(place, values):
    own = jnp.sum(values * values, axis=1)
    total = own
    for s in range(1, place.tps):
        total = total + place.from_tp(own, s)
    return lax.rsqrt(total / (values.shape[1] * place.tps) + epsilon)


def normalize(place, token_rows, gain):
    values = token_rows.astype(jnp.float32)
    return (values * inverse_norm(place, values)[:, None] * gain).astype(low)


def all_features(place, local, width):
    held = jnp.concatenate([local] + [place.from_tp(local, s) for s in range(1, place.tps)], axis=1)
    whole = held.shape[1]
    offsets = [(offset - place.t * local.shape[1]) % whole for offset in place.order(width)]
    return columns(held, offsets, width)


def own_features(place, product, width):
    local = product.shape[1] // place.tps
    count = local // width

    def share(peer):
        return columns(product, [place.position(peer * count + b) * width for b in range(count)], width)

    total = share(place.t)
    for s in range(1, place.tps):
        total = total + place.from_tp(share((place.t - s) % place.tps).astype(low), s).astype(jnp.float32)
    return total


def causal_taps(values, taps):
    tap_count = taps.shape[0]
    grouped = values.reshape(-1, LEN, values.shape[1])
    padded = jnp.pad(grouped, ((0, 0), (tap_count - 1, 0), (0, 0)))
    running = jnp.zeros_like(grouped)
    for offset in range(tap_count):
        running = running + taps[offset] * padded[:, offset : offset + LEN]
    return running.reshape(values.shape)


def dot(left, right):
    return jnp.dot(left, right, preferred_element_type=jnp.float32)


def per_device(
    tokens, mixer_gain, outer_weight, inner_weight, value_weight, outer_scale, inner_scale,
    value_scale, mixer_taps, mixer_project, project_scale, channel_gain, gate_weight, gate_scale,
    up_weight, up_scale, channel_taps, channel_bias, down_weight, down_scale,
):
    sizes = Sizes(
        tuple(lax.axis_size(a) for a in ("rep", "fs", "tp")), tokens, outer_weight, gate_weight, mixer_project
    )
    if sizes.fits(mixer_project):
        return in_one_kernel(
            sizes, tokens, mixer_gain, outer_weight, inner_weight, value_weight, outer_scale, inner_scale,
            value_scale, mixer_taps, mixer_project, project_scale, channel_gain, gate_weight, gate_scale,
            up_weight, up_scale, channel_taps, channel_bias, down_weight, down_scale,
        )
    place = Place()
    rows = outer_weight.shape[0] // place.reps
    width = mixer_project.shape[1] // place.reps
    slow = place.slow
    quarter = gate_weight.shape[1] // slow

    def row_share(weight):
        return lax.dynamic_slice_in_dim(weight, place.r * rows, rows, 0).astype(low)

    def column_share(weight):
        return lax.dynamic_slice_in_dim(weight, place.r * width, width, 1).astype(low)

    def same(piece):
        return [piece] + [place.from_slow(piece, k) for k in range(1, slow)]

    def exchange(take):
        return [take(place.z)] + [
            place.from_slow(take((place.z - k) % slow), k) for k in range(1, slow)
        ]

    mixer_in = place.spread(
        same(jnp.concatenate([row_share(w) for w in (outer_weight, inner_weight, value_weight)], axis=1)), 0
    )
    project = place.spread(same(column_share(mixer_project)), 1)

    def column_part(weight):
        parts = row_share(weight).reshape(rows, slow, quarter).transpose(1, 0, 2)
        return lambda z: lax.dynamic_index_in_dim(parts, z, 0, keepdims=False)

    gate_full = place.spread(exchange(column_part(gate_weight)), 0)
    up_full = place.spread(exchange(column_part(up_weight)), 0)
    down_share = column_share(down_weight)
    down_full = place.spread(
        exchange(lambda z: lax.dynamic_slice_in_dim(down_share, z * quarter, quarter, 0)), 1
    )

    scales = (outer_scale, inner_scale, value_scale, gate_scale, up_scale, project_scale, down_scale)
    packed = lax.all_gather(jnp.concatenate(scales), "fs", axis=0)
    ends, full = 0, []
    for scale in scales:
        full.append(packed[:, ends : ends + scale.shape[0]].reshape(-1))
        ends += scale.shape[0]
    outer_all, inner_all, value_all, gate_all, up_all, project_all, down_all = full
    local = tokens.shape[1]

    def mine(vector, at, size):
        return lax.dynamic_slice_in_dim(vector, at * size, size, vector.ndim - 1)

    normed = all_features(place, normalize(place, tokens, mixer_gain), rows)
    parts = dot(normed, mixer_in)
    each = outer_weight.shape[1]
    outer_part = parts[:, :each] * outer_all
    conv_input = parts[:, each : 2 * each] * inner_all * (parts[:, 2 * each :] * value_all)
    mixed = (outer_part * causal_taps(conv_input, mixer_taps)).astype(low)
    mixer_sum = own_features(place, dot(mixed, project), width) * mine(project_all, place.t, local)
    middle = (tokens.astype(jnp.float32) + mixer_sum).astype(low)

    normed_own = normalize(place, middle, channel_gain)
    normed_two = jnp.concatenate(
        [normed_own] + [place.from_slow(normed_own, k) for k in range(1, slow)], axis=0
    )
    normed_two = all_features(place, normed_two, rows)
    gate_part = dot(normed_two, gate_full) * mine(gate_all, place.z, quarter)
    up_part = dot(normed_two, up_full) * mine(up_all, place.z, quarter)
    hidden = (
        jax.nn.silu(
            causal_taps(gate_part, mine(channel_taps, place.z, quarter))
            + mine(channel_bias, place.z, quarter)
        )
        * up_part
    ).astype(low)
    share = own_features(place, dot(hidden, down_full), width)
    count = tokens.shape[0]
    total = share[:count]
    for k in range(1, slow):
        sent = share[k * count : (k + 1) * count].astype(low)
        total = total + place.from_slow(sent, -k).astype(jnp.float32)
    return (middle.astype(jnp.float32) + total * mine(down_all, place.t, local)).astype(low)


class Sizes:
    def __init__(self, mesh_sizes, tokens, outer_weight, gate_weight, mixer_project):
        self.reps, self.fs, self.tps = mesh_sizes
        self.rows, self.half = tokens.shape
        self.depth, self.cols = outer_weight.shape
        self.block = self.depth // 2
        self.chan = self.cols // 2
        self.quarter = gate_weight.shape[1] // GROUPS
        self.full = self.quarter // LANES
        self.tail = self.quarter % LANES
        self.padded = (self.full + 1) * LANES
        self.wide = 2 * self.quarter
        self.per_half = self.fs // 2
        self.features = self.half * self.tps

    def fits(self, mixer_project):
        return (
            (self.reps, self.fs, self.tps) == (2, 2 * GROUPS, 2)
            and self.rows == LEN
            and self.depth % (2 * LANES) == 0
            and self.per_half * self.depth == self.half
            and self.cols % (4 * LANES) == 0
            and self.tail == LANES // 2
            and self.quarter % 32 == 0
            and mixer_project.shape[1] == self.depth
        )


def layer_kernel(
    n, tok_h, mg, cg, mt, ct, pk, ow, iw, vw, pw, gw, uw, dn, out,
    tok, st_m, st_p, st_g, st_u, st_d, mi, pj, msi, msp, gu, dw, sg, sd, sc, gsus, sq, sqr,
    xg, mps, mpr, ys, yr, mid, ng, hid, acc, ps, pr, zs, zb, za, lsem, ss, rs,
):
    f32 = jnp.float32
    zn = GROUPS
    r, f, t = lax.axis_index("rep"), lax.axis_index("fs"), lax.axis_index("tp")
    z, y = f // 2, f % 2
    py, px, pt = (r, f + 1 - 2 * y, t), (1 - r, f, t), (r, f, 1 - t)
    fy = 2 * z + 1 - y
    up, down = (r, (f + 2) % n.fs, t), (r, (f + n.fs - 2) % n.fs, t)
    can_up, can_down = z < zn - 1, z > 0
    D, B, CH, Q = n.depth, n.block, n.chan, n.quarter

    used = [0]
    pending = []

    def ids(count=1):
        used[0] += count
        return used[0] - count

    def when(cond, fn):
        if cond is None:
            fn()
        else:
            pl.when(cond)(fn)

    def send(src, dst, sid, rid, dev, cond=None):
        c = pltpu.make_async_remote_copy(
            src_ref=src, dst_ref=dst, send_sem=ss.at[sid], recv_sem=rs.at[rid],
            device_id=dev, device_id_type=MESH,
        )
        when(cond, c.start)
        pending.append((c, cond))

    def arrive(dst, rid, cond=None):
        c = pltpu.make_async_remote_copy(
            src_ref=dst, dst_ref=dst, send_sem=ss.at[0], recv_sem=rs.at[rid],
            device_id=pt, device_id_type=MESH,
        )
        when(cond, c.wait_recv)

    def place(fb, rh):
        return pl.multiple_of((fb // n.per_half) * n.half + rh * (n.half // 2) + (fb % n.per_half) * B, B)

    def dot(a, b):
        return jnp.dot(a, b, preferred_element_type=f32)

    def conv(v, w0, w1, w2):
        at = lax.broadcasted_iota(jnp.int32, v.shape, 0)
        one = jnp.where(at >= 1, pltpu.roll(v, 1, axis=0), 0.0)
        two = jnp.where(at >= 2, pltpu.roll(v, 2, axis=0), 0.0)
        return w0 * two + w1 * one + w2 * v

    loads = []

    def load(src, dst):
        c = pltpu.make_async_copy(src, dst, lsem.at[len(loads)])
        c.start()
        loads.append(c)
        return c

    load_tok = load(tok_h, tok)
    load_m = []
    for m, w in enumerate((ow, iw, vw)):
        for h in range(2):
            load_m.append(load(w.at[:, h * CH:(h + 1) * CH], st_m.at[m, h]))
    load_m.append(load(pw, st_p))
    load_f = [load(gw, st_g), load(uw, st_u), load(dn, st_d)]

    barrier = pltpu.get_barrier_semaphore()
    for k in range(1, n.fs):
        pl.semaphore_signal(barrier, inc=1, device_id=(r, (f + k) % n.fs, t), device_id_type=MESH)
    pl.semaphore_signal(barrier, inc=1, device_id=px, device_id_type=MESH)
    pl.semaphore_signal(barrier, inc=1, device_id=pt, device_id_type=MESH)
    pl.semaphore_wait(barrier, n.fs + 1)

    load_tok.wait()

    def square_sum(values):
        return jnp.sum(values * values, axis=1, keepdims=True)

    sq_id = ids(2)

    def share_squares(which, total):
        sq[which] = jnp.broadcast_to(total, (n.rows, LANES))
        send(sq.at[which], sqr.at[which], sq_id + which, sq_id + which, pt)

    share_squares(0, square_sum(tok[...].astype(f32)))

    for c in load_m:
        c.wait()
    m1 = ids(4)
    for m in range(3):
        msi[:, m * CH:(m + 1) * CH] = st_m[m, 1 - y].astype(low)
    for rh in range(2):
        msp[rh] = st_p[pl.ds(pl.multiple_of((1 - y) * CH + rh * (CH // 2), CH // 2), CH // 2), :].astype(low)

    def send_m1(rh):
        here = pl.ds(pl.multiple_of(rh * B, B), B)
        send(msi.at[here], mi.at[pl.ds(place(f, rh), B)], m1 + rh, m1 + rh, py)
        send(msp.at[rh], pj.at[rh, f], m1 + 2 + rh, m1 + 2 + rh, py)

    def arrive_m1(rh):
        arrive(mi.at[pl.ds(place(fy, rh), B)], m1 + rh)
        arrive(pj.at[rh, fy], m1 + 2 + rh)

    send_m1(r)
    for rh in range(2):
        for m in range(3):
            mi[pl.ds(place(f, rh), B), m * CH:(m + 1) * CH] = st_m[m, y, rh * B:(rh + 1) * B, :].astype(low)
        pj[rh, f] = st_p[pl.ds(pl.multiple_of(y * CH + rh * (CH // 2), CH // 2), CH // 2), :].astype(low)

    def normalize(values, which, own, gain, dst):
        arrive(sqr.at[which], sq_id + which)
        total = own + sqr[which][:, :1]
        inverse = lax.rsqrt(total / n.features + epsilon)
        for fl in range(n.per_half):
            for rh in range(2):
                here = slice((2 * fl + rh) * B, (2 * fl + rh + 1) * B)
                there = slice((rh * n.per_half + fl) * B, (rh * n.per_half + fl + 1) * B)
                dst[:, there] = (values[:, here].astype(f32) * inverse * gain[:, here]).astype(low)

    normalize(tok, 0, sq[0][:, :1], mg, xg.at[y, t])
    x_y, x_t = ids(), ids(2)
    send(xg.at[y, t], xg.at[y, t], x_y, x_y, py)
    send(xg.at[y, t], xg.at[y, t], x_t, x_t, pt)
    send_m1(1 - r)

    scale_s, scale_r = ids(n.fs), ids(n.fs)
    sc[f] = pk[...]
    for k in range(1, n.fs):
        send(pk, sc.at[f], scale_s + k, scale_r + f, (r, (f + k) % n.fs, t))

    class Line:
        def __init__(self, blocks):
            self.blocks = blocks
            self.count = len(blocks(0))
            self.up, self.down = ids(zn * self.count), ids(zn * self.count)
            self.below, self.above = ids(zn * self.count), ids(zn * self.count)

        def forward(self, at, k, upward, cond):
            base_s = self.up if upward else self.down
            base_r = self.below if upward else self.above
            for i, b in enumerate(self.blocks(at)):
                send(b, b, base_s + k * self.count + i, base_r + (k + 1) * self.count + i,
                     up if upward else down, cond)

        def start(self):
            self.forward(z, 0, True, can_up)
            self.forward(z, 0, False, can_down)

        def step(self, k, then):
            a, b = (z + zn - k) % zn, (z + k) % zn
            for at, base, upward, cond, more in (
                (a, self.below, True, z >= k, can_up), (b, self.above, False, z < zn - k, can_down),
            ):
                for i, blk in enumerate(self.blocks(at)):
                    arrive(blk, base + k * self.count + i, cond)
                if k < zn - 1:
                    self.forward(at, k, upward, cond & more)
                then(at, k, upward, cond)

    def mixer_blocks(rh):
        def blocks(at):
            pair = 2 * at
            return [mi.at[pl.ds(place(pair, rh), 2 * B)], pj.at[rh, pl.ds(pair, 2)]]
        return blocks

    arrive_m1(r)
    mixer_line = Line(mixer_blocks(r))
    mixer_line.start()
    mx = ids(4 * zn)

    def mixer_over_x(at, k, upward, cond):
        for i, b in enumerate(mixer_blocks(r)(at)):
            s = mx + 4 * k + (2 if upward else 0) + i
            send(b, b, s, s, px, cond)

    for c in load_f:
        c.wait()

    def tiles(rows, q):
        base = q * Q // LANES * LANES
        g = st_g[rows, base:base + n.padded]
        u = st_u[rows, base:base + n.padded]
        if q * Q % LANES:
            g = pltpu.roll(g, n.padded - LANES // 2, axis=1)
            u = pltpu.roll(u, n.padded - LANES // 2, axis=1)
        parts = []
        for j in range(n.full):
            parts += [g[:, j * LANES:(j + 1) * LANES], u[:, j * LANES:(j + 1) * LANES]]
        lane = lax.broadcasted_iota(jnp.int32, (B, LANES), 1)
        parts.append(jnp.where(lane < LANES // 2, g[:, n.full * LANES:], pltpu.roll(u[:, n.full * LANES:], LANES // 2, axis=1)))
        return parts

    for q in range(zn):
        @pl.when(z == q)
        def _():
            for rh in range(2):
                for j, piece in enumerate(tiles(pl.ds(rh * B, B), q)):
                    gu[pl.ds(place(f, rh), B), j * LANES:(j + 1) * LANES] = piece.astype(low)

        @pl.when(z != q)
        def _():
            for j, piece in enumerate(tiles(pl.ds(pl.multiple_of(r * B, B), B), q)):
                sg[q, :, j * LANES:(j + 1) * LANES] = piece.astype(low)

        sd[q] = st_d[pl.ds(pl.multiple_of(q * Q + r * (Q // 2), 16), Q // 2), :].astype(low)
    dw[f] = st_d[pl.ds(pl.multiple_of(z * Q, 16), Q), :].astype(low)

    def gu_at(fb, rh):
        return gu.at[pl.ds(place(fb, rh), B)]

    def dw_at(fb, rh):
        return dw.at[fb, pl.ds(pl.multiple_of(rh * (Q // 2), 16), Q // 2)]

    fy_own = ids(3)
    for rh in range(2):
        send(gu_at(f, rh), gu_at(f, rh), fy_own + rh, fy_own + rh, py)
    send(dw.at[f], dw.at[f], fy_own + 2, fy_own + 2, py)

    arrive(xg.at[1 - y, t], x_y)
    send(xg.at[1 - y, t], xg.at[1 - y, t], x_t + 1, x_t + 1, pt)

    f1, f2y, f2x, f2d = ids(2 * zn), ids(2 * zn), ids(2 * zn), ids(2 * zn)

    def across(k):
        if k == 1:
            return z + 1 - 2 * (z % 2)
        if k == 2:
            return z + 2 - 4 * (z // 2)
        return zn - 1 - z

    def stage_one(k):
        q = across(k)
        dev = (r, 2 * q + y, t)
        send(sg.at[q], gu_at(f, r), f1 + 2 * k, f1 + 2 * k, dev)
        send(sd.at[q], dw_at(f, r), f1 + 2 * k + 1, f1 + 2 * k + 1, dev)

    def stage_two(k):
        fb = 2 * across(k) + y
        for i, ref in enumerate((gu_at(fb, r), dw_at(fb, r))):
            arrive(ref, f1 + 2 * k + i)
            send(ref, ref, f2y + 2 * k + i, f2y + 2 * k + i, py)
            send(ref, ref, f2x + 2 * k + i, f2x + 2 * k + i, px)

    def stage_three(k):
        fb = 2 * across(k) + 1 - y
        for i, ref in enumerate((gu_at(fb, r), dw_at(fb, r))):
            arrive(ref, f2y + 2 * k + i)
            send(ref, ref, f2d + 2 * k + i, f2d + 2 * k + i, px)

    def stage_end(k):
        for base, fb in ((f2x, 2 * across(k) + y), (f2d, 2 * across(k) + 1 - y)):
            for i, ref in enumerate((gu_at(fb, 1 - r), dw_at(fb, 1 - r))):
                arrive(ref, base + 2 * k + i)

    mixer_line.step(1, mixer_over_x)
    mixer_line.step(2, mixer_over_x)
    for k in range(1, zn):
        stage_one(k)
    mixer_line.step(3, mixer_over_x)

    for k in range(1, n.fs):
        fk = (f + k) % n.fs
        arrive(sc.at[fk], scale_r + fk)
    lanes = 3 * CH
    for i in range(2):
        here = slice(lanes + i * n.padded, lanes + (i + 1) * n.padded)
        gsus[i:i + 1, :] = sc[2 * z][:, here] + sc[2 * z + 1][:, here]
    out_at = lanes + 2 * n.padded
    arrive_m1(1 - r)
    for i in range(2):
        arrive(xg.at[y if i == 0 else 1 - y, 1 - t], x_t + i)
    for k in range(1, zn):
        for side, at, cond in ((2, (z + zn - k) % zn, z >= k), (0, (z + k) % zn, z < zn - k)):
            for i, b in enumerate(mixer_blocks(1 - r)(at)):
                arrive(b, mx + 4 * k + side + i, cond)

    scale = [
        sum((sc[n.per_half * y + j][:, m * CH:(m + 1) * CH] for j in range(1, n.per_half)),
            sc[n.per_half * y][:, m * CH:(m + 1) * CH])
        for m in range(3)
    ]
    mt_id, my_id = ids(2), ids()

    def wide(fl):
        return slice(fl * D, (fl + 1) * D)

    for i, sy in enumerate((1 - y, y)):
        def part(m):
            here = slice(m * CH, (m + 1) * CH)
            return (dot(xg[sy, 0], mi[:n.half, here]) + dot(xg[sy, 1], mi[n.half:, here])) * scale[m]

        cv = conv(part(1) * part(2), mt[0:1, :], mt[1:2, :], mt[2:3, :])
        mixed = (part(0) * cv).astype(low)

        def project(fb):
            return dot(mixed[:, :CH // 2], pj[0, fb]) + dot(mixed[:, CH // 2:], pj[1, fb])

        for fl in range(n.per_half):
            mps[i, :, wide(fl)] = project(n.per_half * (1 - t) + fl).astype(low)
        send(mps.at[i], mpr.at[i], mt_id + i, mt_id + i, pt)
        for fl in range(n.per_half):
            acc[i, :, wide(fl)] = project(n.per_half * t + fl)
        if i == 0:
            arrive(mpr.at[0], mt_id)
            ys[...] = (acc[0] + mpr[0].astype(f32)).astype(low)
            send(ys, yr, my_id, my_id, py)
    arrive(mpr.at[1], mt_id + 1)

    stage_two(1)

    arrive(yr, my_id)
    total_sq = None
    for fl in range(n.per_half):
        w = wide(fl)
        added = (acc[1, :, w] + mpr[1, :, w].astype(f32) + yr[:, w].astype(f32)) * sc[n.per_half * t + fl][:, out_at:out_at + D]
        middle = (tok[:, w].astype(f32) + added).astype(low)
        mid[:, w] = middle
        part_sq = square_sum(middle.astype(f32))
        total_sq = part_sq if total_sq is None else total_sq + part_sq
    share_squares(1, total_sq)
    normalize(mid, 1, total_sq, cg, ng.at[z, t])

    token_line = Line(lambda at: [ng.at[at, t]])
    token_line.start()
    n_t = ids(2 * zn)
    send(ng.at[z, t], ng.at[z, t], n_t, n_t, pt)

    def to_core(at, k, upward, cond):
        s = n_t + 2 * k + (1 if upward else 0)
        send(ng.at[at, t], ng.at[at, t], s, s, pt, cond)

    stage_two(2)
    stage_three(1)
    token_line.step(1, to_core)
    stage_two(3)
    stage_three(2)
    token_line.step(2, to_core)
    stage_three(3)
    token_line.step(3, to_core)

    arrive(ng.at[z, 1 - t], n_t)
    for k in range(1, zn):
        for side, at, cond in ((1, (z + zn - k) % zn, z >= k), (0, (z + k) % zn, z < zn - k)):
            arrive(ng.at[at, 1 - t], n_t + 2 * k + side, cond)
    for rh in range(2):
        arrive(gu_at(fy, rh), fy_own + rh)
    arrive(dw.at[fy], fy_own + 2)
    for k in range(1, zn):
        stage_end(k)

    p_t, z_s, z_b, z_a = ids(zn), ids(zn), ids(zn), ids(zn)
    side = z // 2
    order = (3 * (1 - side), 2 - side, z + 1 - 2 * (z % 2), z)
    inner = (z > 0) & (z < zn - 1)

    def to_line(i, s, cond_up, cond_down):
        send(zs.at[s], zb.at[s], z_s + i, z_b + s, up, cond_up)
        send(zs.at[s], za.at[s], z_s + i, z_a + s, down, cond_down)

    for i, s in enumerate(order):
        def gated(a, here):
            c = conv(a * gsus[0:1, here], ct[0:1, here], ct[1:2, here], ct[2:3, here]) + ct[3:4, here]
            return c / (1.0 + jnp.exp(-c))

        def product(at, width):
            here = pl.ds(at, width)
            return dot(ng[s, 0], gu[:n.half, here]) + dot(ng[s, 1], gu[n.half:, here])

        def tile(j, carry):
            a = product(pl.multiple_of(j * 2 * LANES, 2 * LANES), 2 * LANES)
            here = pl.ds(pl.multiple_of(j * LANES, LANES), LANES)
            hid[:, here] = (gated(a[:, :LANES], here) * (a[:, LANES:] * gsus[1:2, here])).astype(low)
            return carry

        lax.fori_loop(0, n.full, tile, 0)
        a = product(n.full * 2 * LANES, LANES)
        here = slice(n.full * LANES, n.padded)
        last = gated(a, here) * (pltpu.roll(a, LANES // 2, axis=1) * gsus[1:2, here])
        hid[:, n.full * LANES:] = last.astype(low)[:, :n.tail]
        hid_v = hid[...]
        for fl in range(n.per_half):
            ps[i, :, wide(fl)] = dot(hid_v, dw[n.per_half * (1 - t) + fl]).astype(low)
        send(ps.at[i], pr.at[i], p_t + i, p_t + i, pt)
        for fl in range(n.per_half):
            acc[i, :, wide(fl)] = dot(hid_v, dw[n.per_half * t + fl])
        arrive(pr.at[i], p_t + i)
        acc[i] = acc[i] + pr[i].astype(f32)
        if i < zn - 1:
            @pl.when(z == 0)
            def _():
                zs[s] = acc[i].astype(low)

            @pl.when(z == zn - 1)
            def _():
                zs[s] = acc[i].astype(low)

            to_line(i, s, z == 0, z == zn - 1)

    for i, s in enumerate(order[:zn - 1]):
        go_up, go_down = inner & (s > z), inner & (s < z)
        arrive(zb.at[s], z_b + s, go_up)
        arrive(za.at[s], z_a + s, go_down)

        @pl.when(go_up)
        def _():
            zs[s] = (acc[i] + zb[s].astype(f32)).astype(low)

        @pl.when(go_down)
        def _():
            zs[s] = (acc[i] + za[s].astype(f32)).astype(low)

        to_line(i, s, go_up, go_down)

    arrive(zb.at[z], z_b + z, can_down)

    @pl.when(can_down)
    def _():
        acc[zn - 1] = acc[zn - 1] + zb[z].astype(f32)

    arrive(za.at[z], z_a + z, can_up)

    @pl.when(can_up)
    def _():
        acc[zn - 1] = acc[zn - 1] + za[z].astype(f32)

    for fl in range(n.per_half):
        w = wide(fl)
        scaled = acc[zn - 1, :, w] * sc[n.per_half * t + fl][:, out_at + D:out_at + 2 * D]
        out[:, w] = (mid[:, w].astype(f32) + scaled).astype(low)

    for c, cond in pending:
        when(cond, c.wait_send)
    assert used[0] <= SEMAPHORES, used[0]


def in_one_kernel(
    n, tokens, mixer_gain, outer_weight, inner_weight, value_weight, outer_scale, inner_scale,
    value_scale, mixer_taps, mixer_project, project_scale, channel_gain, gate_weight, gate_scale,
    up_weight, up_scale, channel_taps, channel_bias, down_weight, down_scale,
):
    f = lax.axis_index("fs")
    z, y = f // 2, f % 2
    f32, zn = jnp.float32, GROUPS

    def spaced(vector, at, parts, padded):
        size = vector.shape[0]
        tiled = jnp.where(jnp.arange(parts * size) // size == at, jnp.tile(vector, parts), 0.0)
        return jnp.pad(tiled, (0, padded - parts * size))

    packed = jnp.concatenate(
        [spaced(v, f % n.per_half, n.per_half, n.chan) for v in (outer_scale, inner_scale, value_scale)]
        + [spaced(v, y, 2, n.padded) for v in (gate_scale, up_scale)]
        + [project_scale, down_scale]
    )[None, :]
    taps = lax.dynamic_slice_in_dim(mixer_taps, y * n.chan, n.chan, 1)
    gate_taps = jnp.concatenate([channel_taps, channel_bias[None, :]], axis=0)
    gate_taps = lax.dynamic_slice_in_dim(gate_taps, z * n.quarter, n.quarter, 1)
    gate_taps = jnp.pad(gate_taps, ((0, 0), (0, n.padded - n.quarter)))

    vm, anywhere = pl.BlockSpec(memory_space=pltpu.VMEM), pl.BlockSpec(memory_space=pl.ANY)
    rows, half, features = n.rows, n.half, n.features

    def V(shape, dtype=low):
        return pltpu.VMEM(shape, dtype)

    scratch = [
        V((rows, half)),
        V((3, 2, n.depth, n.chan), f32), V((n.cols, n.depth), f32),
        V((n.depth, zn * n.quarter), f32), V((n.depth, zn * n.quarter), f32), V((zn * n.quarter, n.depth), f32),
        V((features, 3 * n.chan)), V((2, n.fs, n.chan // 2, n.depth)),
        V((n.depth, 3 * n.chan)), V((2, n.chan // 2, n.depth)),
        V((features, n.wide)), V((n.fs, n.quarter, n.depth)),
        V((zn, n.block, n.wide)), V((zn, n.quarter // 2, n.depth)),
        V((n.fs,) + packed.shape, f32), V((2, n.padded), f32),
        V((2, rows, LANES), f32), V((2, rows, LANES), f32),
        V((2, 2, rows, half)), V((2, rows, half)), V((2, rows, half)), V((rows, half)), V((rows, half)),
        V((rows, half)), V((zn, 2, rows, half)), V((rows, n.quarter)), V((zn, rows, half), f32),
        V((zn, rows, half)), V((zn, rows, half)), V((zn, rows, half)), V((zn, rows, half)), V((zn, rows, half)),
        pltpu.SemaphoreType.DMA((16,)), pltpu.SemaphoreType.DMA((SEMAPHORES,)), pltpu.SemaphoreType.DMA((SEMAPHORES,)),
    ]
    return pl.pallas_call(
        functools.partial(layer_kernel, n),
        out_shape=jax.ShapeDtypeStruct(tokens.shape, tokens.dtype),
        in_specs=[anywhere] + [vm] * 5 + [anywhere] * 7,
        out_specs=vm,
        scratch_shapes=scratch,
        compiler_params=pltpu.CompilerParams(
            collective_id=0, has_side_effects=True, vmem_limit_bytes=VMEM_BYTES
        ),
    )(
        tokens, mixer_gain[None, :], channel_gain[None, :], taps, gate_taps, packed,
        outer_weight, inner_weight, value_weight, mixer_project, gate_weight, up_weight, down_weight,
    )


def solution(mesh):
    placed = (
        P(("rep", "fs"), "tp"),
        P("tp"),
        P("fs", "tp"),
        P("fs", "tp"),
        P("fs", "tp"),
        P(("tp", "fs")),
        P(("tp", "fs")),
        P(("tp", "fs")),
        P(None, "tp"),
        P("tp", "fs"),
        P("fs"),
        P("tp"),
        P("fs", "tp"),
        P(("tp", "fs")),
        P("fs", "tp"),
        P(("tp", "fs")),
        P(None, "tp"),
        P("tp"),
        P("tp", "fs"),
        P("fs"),
    )
    return jax.shard_map(
        per_device, mesh=mesh, in_specs=placed, out_specs=P(("rep", "fs"), "tp"), check_vma=False
    )
```

```python
import functools

import jax
import jax.numpy as jnp
from jax import lax
from jax.experimental import pallas as pl
from jax.experimental.pallas import tpu as pltpu
from jax.sharding import PartitionSpec as P

LEN = 320
GROUPS = 4
LANES = 128
SEMAPHORES = 256
VMEM_BYTES = 65000 * 1024
MESH = pl.DeviceIdType.MESH

epsilon = 1e-06
low = jnp.bfloat16


class Place:
    def __init__(self):
        self.fs = lax.axis_size("fs")
        self.reps = lax.axis_size("rep")
        self.tps = lax.axis_size("tp")
        self.slow = GROUPS if self.fs % GROUPS == 0 else 1
        self.fast = self.fs // self.slow
        at = lax.axis_index("fs")
        self.z, self.y = at // self.fast, at % self.fast
        self.r, self.t = lax.axis_index("rep"), lax.axis_index("tp")

    def from_slow(self, block, shift):
        perm = [(z * self.fast + y, (z - shift) % self.slow * self.fast + y)
                for z in range(self.slow) for y in range(self.fast)]
        return lax.ppermute(block, "fs", perm)

    def from_fast(self, block, shift):
        perm = [(z * self.fast + y, z * self.fast + (y - shift) % self.fast)
                for z in range(self.slow) for y in range(self.fast)]
        return lax.ppermute(block, "fs", perm)

    def from_rep(self, block, shift):
        return lax.ppermute(block, "rep", [(i, (i - shift) % self.reps) for i in range(self.reps)])

    def from_tp(self, block, shift):
        return lax.ppermute(block, "tp", [(i, (i - shift) % self.tps) for i in range(self.tps)])

    def spread(self, pieces, axis):
        held = jnp.concatenate(pieces, axis)
        held = jnp.concatenate([held] + [self.from_fast(held, j) for j in range(1, self.fast)], axis)
        return jnp.concatenate([held] + [self.from_rep(held, i) for i in range(1, self.reps)], axis)

    def order(self, width):
        return [
            (((self.z + k) % self.slow * self.fast + (self.y + j) % self.fast) * self.reps
             + (self.r + i) % self.reps) * width
            for i in range(self.reps) for j in range(self.fast) for k in range(self.slow)
        ]

    def position(self, block):
        f, part = block // self.reps, block % self.reps
        i = (part - self.r) % self.reps
        j = (f % self.fast - self.y) % self.fast
        k = (f // self.fast - self.z) % self.slow
        return (i * self.fast + j) * self.slow + k


def columns(values, offsets, width):
    return jnp.concatenate(
        [lax.dynamic_slice(values, (0, offset), (values.shape[0], width)) for offset in offsets], axis=1
    )


def inverse_norm(place, values):
    own = jnp.sum(values * values, axis=1)
    total = own
    for s in range(1, place.tps):
        total = total + place.from_tp(own, s)
    return lax.rsqrt(total / (values.shape[1] * place.tps) + epsilon)


def normalize(place, token_rows, gain):
    values = token_rows.astype(jnp.float32)
    return (values * inverse_norm(place, values)[:, None] * gain).astype(low)


def all_features(place, local, width):
    held = jnp.concatenate([local] + [place.from_tp(local, s) for s in range(1, place.tps)], axis=1)
    whole = held.shape[1]
    offsets = [(offset - place.t * local.shape[1]) % whole for offset in place.order(width)]
    return columns(held, offsets, width)


def own_features(place, product, width):
    local = product.shape[1] // place.tps
    count = local // width

    def share(peer):
        return columns(product, [place.position(peer * count + b) * width for b in range(count)], width)

    total = share(place.t)
    for s in range(1, place.tps):
        total = total + place.from_tp(share((place.t - s) % place.tps).astype(low), s).astype(jnp.float32)
    return total


def causal_taps(values, taps):
    tap_count = taps.shape[0]
    grouped = values.reshape(-1, LEN, values.shape[1])
    padded = jnp.pad(grouped, ((0, 0), (tap_count - 1, 0), (0, 0)))
    running = jnp.zeros_like(grouped)
    for offset in range(tap_count):
        running = running + taps[offset] * padded[:, offset : offset + LEN]
    return running.reshape(values.shape)


def dot(left, right):
    return jnp.dot(left, right, preferred_element_type=jnp.float32)


def per_device(
    tokens, mixer_gain, outer_weight, inner_weight, value_weight, outer_scale, inner_scale,
    value_scale, mixer_taps, mixer_project, project_scale, channel_gain, gate_weight, gate_scale,
    up_weight, up_scale, channel_taps, channel_bias, down_weight, down_scale,
):
    sizes = Sizes(
        tuple(lax.axis_size(a) for a in ("rep", "fs", "tp")), tokens, outer_weight, gate_weight, mixer_project
    )
    if sizes.fits(mixer_project):
        return in_one_kernel(
            sizes, tokens, mixer_gain, outer_weight, inner_weight, value_weight, outer_scale, inner_scale,
            value_scale, mixer_taps, mixer_project, project_scale, channel_gain, gate_weight, gate_scale,
            up_weight, up_scale, channel_taps, channel_bias, down_weight, down_scale,
        )
    place = Place()
    rows = outer_weight.shape[0] // place.reps
    width = mixer_project.shape[1] // place.reps
    slow = place.slow
    quarter = gate_weight.shape[1] // slow

    def row_share(weight):
        return lax.dynamic_slice_in_dim(weight, place.r * rows, rows, 0).astype(low)

    def column_share(weight):
        return lax.dynamic_slice_in_dim(weight, place.r * width, width, 1).astype(low)

    def same(piece):
        return [piece] + [place.from_slow(piece, k) for k in range(1, slow)]

    def exchange(take):
        return [take(place.z)] + [
            place.from_slow(take((place.z - k) % slow), k) for k in range(1, slow)
        ]

    mixer_in = place.spread(
        same(jnp.concatenate([row_share(w) for w in (outer_weight, inner_weight, value_weight)], axis=1)), 0
    )
    project = place.spread(same(column_share(mixer_project)), 1)

    def column_part(weight):
        parts = row_share(weight).reshape(rows, slow, quarter).transpose(1, 0, 2)
        return lambda z: lax.dynamic_index_in_dim(parts, z, 0, keepdims=False)

    gate_full = place.spread(exchange(column_part(gate_weight)), 0)
    up_full = place.spread(exchange(column_part(up_weight)), 0)
    down_share = column_share(down_weight)
    down_full = place.spread(
        exchange(lambda z: lax.dynamic_slice_in_dim(down_share, z * quarter, quarter, 0)), 1
    )

    scales = (outer_scale, inner_scale, value_scale, gate_scale, up_scale, project_scale, down_scale)
    packed = lax.all_gather(jnp.concatenate(scales), "fs", axis=0)
    ends, full = 0, []
    for scale in scales:
        full.append(packed[:, ends : ends + scale.shape[0]].reshape(-1))
        ends += scale.shape[0]
    outer_all, inner_all, value_all, gate_all, up_all, project_all, down_all = full
    local = tokens.shape[1]

    def mine(vector, at, size):
        return lax.dynamic_slice_in_dim(vector, at * size, size, vector.ndim - 1)

    normed = all_features(place, normalize(place, tokens, mixer_gain), rows)
    parts = dot(normed, mixer_in)
    each = outer_weight.shape[1]
    outer_part = parts[:, :each] * outer_all
    conv_input = parts[:, each : 2 * each] * inner_all * (parts[:, 2 * each :] * value_all)
    mixed = (outer_part * causal_taps(conv_input, mixer_taps)).astype(low)
    mixer_sum = own_features(place, dot(mixed, project), width) * mine(project_all, place.t, local)
    middle = (tokens.astype(jnp.float32) + mixer_sum).astype(low)

    normed_own = normalize(place, middle, channel_gain)
    normed_two = jnp.concatenate(
        [normed_own] + [place.from_slow(normed_own, k) for k in range(1, slow)], axis=0
    )
    normed_two = all_features(place, normed_two, rows)
    gate_part = dot(normed_two, gate_full) * mine(gate_all, place.z, quarter)
    up_part = dot(normed_two, up_full) * mine(up_all, place.z, quarter)
    hidden = (
        jax.nn.silu(
            causal_taps(gate_part, mine(channel_taps, place.z, quarter))
            + mine(channel_bias, place.z, quarter)
        )
        * up_part
    ).astype(low)
    share = own_features(place, dot(hidden, down_full), width)
    count = tokens.shape[0]
    total = share[:count]
    for k in range(1, slow):
        sent = share[k * count : (k + 1) * count].astype(low)
        total = total + place.from_slow(sent, -k).astype(jnp.float32)
    return (middle.astype(jnp.float32) + total * mine(down_all, place.t, local)).astype(low)


class Sizes:
    def __init__(self, mesh_sizes, tokens, outer_weight, gate_weight, mixer_project):
        self.reps, self.fs, self.tps = mesh_sizes
        self.rows, self.half = tokens.shape
        self.depth, self.cols = outer_weight.shape
        self.block = self.depth // 2
        self.chan = self.cols // 2
        self.quarter = gate_weight.shape[1] // GROUPS
        self.full = self.quarter // LANES
        self.tail = self.quarter % LANES
        self.padded = (self.full + 1) * LANES
        self.wide = 2 * self.quarter
        self.per_half = self.fs // 2
        self.features = self.half * self.tps
        each = self.chan // self.per_half
        self.slots = [0]
        for width in [each] * 3 + [self.quarter // 2] * 2 + [self.depth] * 2:
            self.slots.append(self.slots[-1] + -(-width // LANES) * LANES)
        self.halves = 2 * each == LANES and 2 * (self.slots[4] - self.slots[3]) == self.padded

    def fits(self, mixer_project):
        return (
            (self.reps, self.fs, self.tps) == (2, 2 * GROUPS, 2)
            and self.rows == LEN
            and self.depth % (2 * LANES) == 0
            and self.per_half * self.depth == self.half
            and self.cols == 4 * self.block
            and self.halves
            and self.tail == LANES // 2
            and self.quarter % 32 == 0
            and mixer_project.shape[1] == self.depth
        )


def layer_kernel(
    n, tok_h, mg, cg, mt, channel_taps, channel_bias, s_o, s_i, s_v, s_g, s_u, s_p, s_d,
    ow, iw, vw, pw, gw, uw, dn, out,
    tok, st_m, st_p, st_g, st_u, st_d, mw, ms, gu, dw, sg, sd, pk, sc, msc, gsus, ct, sq, sqr,
    xg, mps, mpr, ys, yr, mid, ng, hid, acc, ps, pr, zs, zb, za, lsem, ss, rs,
):
    f32 = jnp.float32
    zn = GROUPS
    r, f, t = lax.axis_index("rep"), lax.axis_index("fs"), lax.axis_index("tp")
    z, y = f // 2, f % 2
    py, px, pt = (r, f + 1 - 2 * y, t), (1 - r, f, t), (r, f, 1 - t)
    fy = 2 * z + 1 - y
    up, down = (r, (f + 2) % n.fs, t), (r, (f + n.fs - 2) % n.fs, t)
    can_up, can_down = z < zn - 1, z > 0
    inner = (z > 0) & (z < zn - 1)
    ends = (z == 0) | (z == zn - 1)
    D, B, CH, Q = n.depth, n.block, n.chan, n.quarter

    used = [0]
    pending = []

    def ids(count=1):
        used[0] += count
        return used[0] - count

    def when(cond, fn):
        if cond is None:
            fn()
        else:
            pl.when(cond)(fn)

    def send(src, dst, sid, rid, dev, cond=None):
        c = pltpu.make_async_remote_copy(
            src_ref=src, dst_ref=dst, send_sem=ss.at[sid], recv_sem=rs.at[rid],
            device_id=dev, device_id_type=MESH,
        )
        when(cond, c.start)
        pending.append((c, cond))

    def arrive(dst, rid, cond=None):
        c = pltpu.make_async_remote_copy(
            src_ref=dst, dst_ref=dst, send_sem=ss.at[0], recv_sem=rs.at[rid],
            device_id=pt, device_id_type=MESH,
        )
        when(cond, c.wait_recv)

    def place(fb, rh):
        return pl.multiple_of((fb // n.per_half) * n.half + rh * (n.half // 2) + (fb % n.per_half) * B, B)

    def dot(a, b):
        return jnp.dot(a, b, preferred_element_type=f32)

    def conv(v, w0, w1, w2):
        at = lax.broadcasted_iota(jnp.int32, v.shape, 0)
        one = jnp.where(at >= 1, pltpu.roll(v, 1, axis=0), 0.0)
        two = jnp.where(at >= 2, pltpu.roll(v, 2, axis=0), 0.0)
        return w0 * two + w1 * one + w2 * v

    loads = []

    def load(src, dst):
        c = pltpu.make_async_copy(src, dst, lsem.at[len(loads)])
        c.start()
        loads.append(c)
        return c

    load_tok = load(tok_h, tok)
    load_m = []
    for m, w in enumerate((ow, iw, vw)):
        for h in range(2):
            load_m.append(load(w.at[:, h * CH:(h + 1) * CH], st_m.at[m, h]))
    load_m.append(load(pw, st_p))
    load_f = [load(gw, st_g), load(uw, st_u), load(dn, st_d)]

    barrier = pltpu.get_barrier_semaphore()
    for k in range(1, n.fs):
        pl.semaphore_signal(barrier, inc=1, device_id=(r, (f + k) % n.fs, t), device_id_type=MESH)
    pl.semaphore_signal(barrier, inc=1, device_id=px, device_id_type=MESH)
    pl.semaphore_signal(barrier, inc=1, device_id=pt, device_id_type=MESH)

    for c in load_m:
        c.wait()
    for rh in range(2):
        here = slice(rh * B, (rh + 1) * B)
        for m in range(3):
            ms[here, m * CH:(m + 1) * CH] = st_m[m, 1 - y, here, :].astype(low)
            mw[pl.ds(place(f, rh), B), m * CH:(m + 1) * CH] = st_m[m, y, here, :].astype(low)
        for h, ref, rows in ((1 - y, ms, here), (y, mw, pl.ds(place(f, rh), B))):
            ref[rows, 3 * CH:] = st_p[pl.ds(pl.multiple_of(h * CH + rh * B, B), B), :].astype(low)

    pk[...] = jnp.zeros_like(pk)
    for at, ref in zip(n.slots, (s_o, s_i, s_v, s_g, s_u, s_p, s_d)):
        pk[:, at:at + ref.shape[1]] = ref[...]
    for q in range(zn):
        @pl.when(z == q)
        def _():
            base = q * Q // LANES * LANES
            for ref, rows in ((channel_taps, slice(0, 3)), (channel_bias, slice(3, 4))):
                taps = ref[:, base:base + n.padded]
                ct[rows, :] = pltpu.roll(taps, n.padded - LANES // 2, axis=1) if q * Q % LANES else taps

    load_tok.wait()

    def square_sum(values):
        return jnp.sum(values * values, axis=1, keepdims=True)

    sq_id = ids(2)

    def share_squares(which, total):
        sq[which] = jnp.broadcast_to(total, (n.rows, LANES))
        send(sq.at[which], sqr.at[which], sq_id + which, sq_id + which, pt)

    own_squares = square_sum(tok[...].astype(f32))
    pl.semaphore_wait(barrier, n.fs + 1)
    share_squares(0, own_squares)

    m1 = ids(2)

    def block_at(fb, rh):
        return mw.at[pl.ds(place(fb, rh), B)]

    def send_m1(rh):
        send(ms.at[pl.ds(pl.multiple_of(rh * B, B), B)], block_at(f, rh), m1 + rh, m1 + rh, py)

    def arrive_m1(rh):
        arrive(block_at(fy, rh), m1 + rh)

    send_m1(r)

    class Line:
        def __init__(self, block):
            self.block = block
            self.up, self.down, self.below, self.above = ids(zn), ids(zn), ids(zn), ids(zn)

        def forward(self, at, k, upward, cond):
            b = self.block(at)
            send(b, b, (self.up if upward else self.down) + k, (self.below if upward else self.above) + k + 1,
                 up if upward else down, cond)

        def start(self):
            self.forward(z, 0, True, can_up)
            self.forward(z, 0, False, can_down)

        def step(self, k, then):
            a, b = (z + zn - k) % zn, (z + k) % zn
            for at, base, upward, cond, more in (
                (a, self.below, True, z >= k, can_up), (b, self.above, False, z < zn - k, can_down),
            ):
                arrive(self.block(at), base + k, cond)
                if k < zn - 1:
                    self.forward(at, k, upward, cond & more)
                then(at, k, upward, cond)

    own_line = Line(lambda at: block_at(2 * at + y, r))
    other_line = Line(lambda at: block_at(2 * at + 1 - y, r))
    own_line.start()

    def normalize(values, which, own, gain, dst):
        arrive(sqr.at[which], sq_id + which)
        total = own + sqr[which][:, :1]
        inverse = lax.rsqrt(total / n.features + epsilon)
        for fl in range(n.per_half):
            for rh in range(2):
                here = slice((2 * fl + rh) * B, (2 * fl + rh + 1) * B)
                there = slice((rh * n.per_half + fl) * B, (rh * n.per_half + fl + 1) * B)
                dst[:, there] = (values[:, here].astype(f32) * inverse * gain[:, here]).astype(low)

    normalize(tok, 0, own_squares, mg, xg.at[y, t])
    x_y, x_t = ids(), ids(2)
    send(xg.at[y, t], xg.at[y, t], x_y, x_y, py)
    send(xg.at[y, t], xg.at[y, t], x_t, x_t, pt)
    send_m1(1 - r)

    scale_s, scale_r = ids(n.fs), ids(n.fs)
    sc[f] = pk[...]
    for k in range(1, n.fs):
        send(pk, sc.at[f], scale_s + k, scale_r + f, (r, (f + k) % n.fs, t))

    mx = ids(4 * zn)

    def over_x(which, blk):
        def then(at, k, upward, cond):
            s = mx + 4 * k + 2 * which + (1 if upward else 0)
            send(blk(at), blk(at), s, s, px, cond)
        return then

    for c in load_f:
        c.wait()

    def tiles(rows, q):
        base = q * Q // LANES * LANES
        g = st_g[rows, base:base + n.padded]
        u = st_u[rows, base:base + n.padded]
        if q * Q % LANES:
            g = pltpu.roll(g, n.padded - LANES // 2, axis=1)
            u = pltpu.roll(u, n.padded - LANES // 2, axis=1)
        parts = []
        for j in range(n.full):
            parts += [g[:, j * LANES:(j + 1) * LANES], u[:, j * LANES:(j + 1) * LANES]]
        lane = lax.broadcasted_iota(jnp.int32, (B, LANES), 1)
        parts.append(jnp.where(lane < LANES // 2, g[:, n.full * LANES:], pltpu.roll(u[:, n.full * LANES:], LANES // 2, axis=1)))
        return parts

    for q in range(zn):
        @pl.when(z == q)
        def _():
            for rh in range(2):
                for j, piece in enumerate(tiles(pl.ds(rh * B, B), q)):
                    gu[pl.ds(place(f, rh), B), j * LANES:(j + 1) * LANES] = piece.astype(low)

        @pl.when(z != q)
        def _():
            for j, piece in enumerate(tiles(pl.ds(pl.multiple_of(r * B, B), B), q)):
                sg[q, :, j * LANES:(j + 1) * LANES] = piece.astype(low)

        sd[q] = st_d[pl.ds(pl.multiple_of(q * Q + r * (Q // 2), 16), Q // 2), :].astype(low)
    dw[f] = st_d[pl.ds(pl.multiple_of(z * Q, 16), Q), :].astype(low)

    def gu_at(fb, rh):
        return gu.at[pl.ds(place(fb, rh), B)]

    def dw_at(fb, rh):
        return dw.at[fb, pl.ds(pl.multiple_of(rh * (Q // 2), 16), Q // 2)]

    fy_own = ids(3)
    for rh in range(2):
        send(gu_at(f, rh), gu_at(f, rh), fy_own + rh, fy_own + rh, py)
    send(dw.at[f], dw.at[f], fy_own + 2, fy_own + 2, py)

    f1, f2y, f2x, f2d = ids(2 * zn), ids(2 * zn), ids(2 * zn), ids(2 * zn)

    def across(k):
        if k == 1:
            return z + 1 - 2 * (z % 2)
        if k == 2:
            return z + 2 - 4 * (z // 2)
        return zn - 1 - z

    def stage_one(k, cond):
        q = across(k)
        dev = (r, 2 * q + y, t)
        send(sg.at[q], gu_at(f, r), f1 + 2 * k, f1 + 2 * k, dev, cond)
        send(sd.at[q], dw_at(f, r), f1 + 2 * k + 1, f1 + 2 * k + 1, dev, cond)

    def held(k):
        fb = 2 * across(k) + y
        return enumerate((gu_at(fb, r), dw_at(fb, r)))

    def pieces_over_x(k, cond):
        for i, ref in held(k):
            arrive(ref, f1 + 2 * k + i, cond)
            send(ref, ref, f2x + 2 * k + i, f2x + 2 * k + i, px, cond)

    def pieces_over_y(k):
        for i, ref in held(k):
            send(ref, ref, f2y + 2 * k + i, f2y + 2 * k + i, py)

    def pieces_on(k):
        gates = gu_at(2 * across(k) + 1 - y, r)
        arrive(gates, f2y + 2 * k)
        send(gates, gates, f2d + 2 * k, f2d + 2 * k, px)
        downs = dw_at(2 * across(k) + y, 1 - r)
        arrive(downs, f2x + 2 * k + 1)
        send(downs, downs, f2d + 2 * k + 1, f2d + 2 * k + 1, py)

    def pieces_end(k):
        mine, theirs = 2 * across(k) + y, 2 * across(k) + 1 - y
        arrive(gu_at(mine, 1 - r), f2x + 2 * k)
        arrive(gu_at(theirs, 1 - r), f2d + 2 * k)
        arrive(dw_at(theirs, r), f2y + 2 * k + 1)
        arrive(dw_at(theirs, 1 - r), f2d + 2 * k + 1)

    arrive_m1(r)
    other_line.start()
    stage_one(1, ends)
    own_x, other_x = over_x(0, own_line.block), over_x(1, other_line.block)
    own_line.step(1, own_x)
    other_line.step(1, other_x)
    own_line.step(2, own_x)
    arrive(xg.at[1 - y, t], x_y)
    send(xg.at[1 - y, t], xg.at[1 - y, t], x_t + 1, x_t + 1, pt)
    other_line.step(2, other_x)
    stage_one(2, ends)
    stage_one(3, inner)
    stage_one(1, inner)
    own_line.step(3, own_x)
    other_line.step(3, other_x)
    stage_one(3, ends)

    for k in range(1, n.fs):
        fk = (f + k) % n.fs
        arrive(sc.at[fk], scale_r + fk)
    for m, at in enumerate(n.slots[:3]):
        slot = slice(at, at + LANES)
        for j in range(CH // LANES):
            fb = n.per_half * y + 2 * j
            msc[m:m + 1, j * LANES:(j + 1) * LANES] = sc[fb][:, slot] + pltpu.roll(sc[fb + 1][:, slot], LANES // 2, axis=1)
    for i, at in enumerate(n.slots[3:5]):
        first, second = (
            jnp.concatenate([sc[2 * z + h][:, at:at + n.padded // 2], jnp.zeros((1, n.padded // 2), f32)], axis=1)
            for h in range(2)
        )
        gsus[i:i + 1, :] = first + pltpu.roll(second, Q // 2, axis=1)
    arrive_m1(1 - r)
    for i in range(2):
        arrive(xg.at[y if i == 0 else 1 - y, 1 - t], x_t + i)
    near = z // 2

    def arrive_mixer(k, own_half):
        for side, at, cond in ((1, (z + zn - k) % zn, z >= k), (0, (z + k) % zn, z < zn - k)):
            for which, fb in enumerate((2 * at + y, 2 * at + 1 - y)):
                same = at // 2 == near
                arrive(block_at(fb, 1 - r), mx + 4 * k + 2 * which + side, cond & (same if own_half else ~same))

    arrive_mixer(1, True)
    near_rows = pl.ds(pl.multiple_of(near * n.half, n.half), n.half)
    far_rows = pl.ds(pl.multiple_of((1 - near) * n.half, n.half), n.half)
    for i, sy in enumerate((1 - y, y)):
        for m in range(3):
            here = slice(m * CH, (m + 1) * CH)
            acc[2 + i, :, here] = dot(xg[sy, near], mw[near_rows, here])
    for k in range(1, zn):
        arrive_mixer(k, False)
    stage_one(2, inner)

    y_lanes = pl.ds(pl.multiple_of(y * CH, CH), CH)
    m_taps = [mt[k:k + 1, y_lanes] for k in range(3)]
    mt_id, my_id = ids(2), ids()

    def wide(fl):
        return slice(fl * D, (fl + 1) * D)

    for i, sy in enumerate((1 - y, y)):
        def part(m):
            here = slice(m * CH, (m + 1) * CH)
            return (acc[2 + i, :, here] + dot(xg[sy, 1 - near], mw[far_rows, here])) * msc[m:m + 1, :]

        cv = conv(part(1) * part(2), *m_taps)
        mixed = (part(0) * cv).astype(low)

        def project(fb):
            return dot(mixed, jnp.concatenate([mw[pl.ds(place(fb, rh), B), 3 * CH:] for rh in range(2)], axis=0))

        for fl in range(n.per_half):
            mps[i, :, wide(fl)] = project(n.per_half * (1 - t) + fl).astype(low)
        send(mps.at[i], mpr.at[i], mt_id + i, mt_id + i, pt)
        for fl in range(n.per_half):
            acc[i, :, wide(fl)] = project(n.per_half * t + fl)
        if i == 0:
            arrive(mpr.at[0], mt_id)
            ys[...] = (acc[0] + mpr[0].astype(f32)).astype(low)
            send(ys, yr, my_id, my_id, py)
            pieces_over_x(1, inner)
    arrive(mpr.at[1], mt_id + 1)

    pieces_over_x(3, inner)
    pieces_over_x(2, inner)
    pieces_over_x(1, ends)

    arrive(yr, my_id)
    total_sq = None
    for fl in range(n.per_half):
        w = wide(fl)
        added = (acc[1, :, w] + mpr[1, :, w].astype(f32) + yr[:, w].astype(f32)) * sc[n.per_half * t + fl][:, n.slots[5]:n.slots[5] + D]
        middle = (tok[:, w].astype(f32) + added).astype(low)
        mid[:, w] = middle
        part_sq = square_sum(middle.astype(f32))
        total_sq = part_sq if total_sq is None else total_sq + part_sq
    share_squares(1, total_sq)
    normalize(mid, 1, total_sq, cg, ng.at[z, t])

    token_line = Line(lambda at: ng.at[at, t])
    token_line.start()
    n_t = ids(2 * zn)
    send(ng.at[z, t], ng.at[z, t], n_t, n_t, pt)

    def to_core(at, k, upward, cond):
        s = n_t + 2 * k + (1 if upward else 0)
        send(ng.at[at, t], ng.at[at, t], s, s, pt, cond)

    pieces_over_y(1)
    for k in (2, 3):
        pieces_over_x(k, ends)
        pieces_over_y(k)
    pieces_on(1)
    token_line.step(1, to_core)
    pieces_on(2)
    token_line.step(2, to_core)
    pieces_on(3)
    token_line.step(3, to_core)

    arrive(ng.at[z, 1 - t], n_t)
    for k in range(1, zn):
        for side, at, cond in ((1, (z + zn - k) % zn, z >= k), (0, (z + k) % zn, z < zn - k)):
            arrive(ng.at[at, 1 - t], n_t + 2 * k + side, cond)
    for rh in range(2):
        arrive(gu_at(fy, rh), fy_own + rh)
    arrive(dw.at[fy], fy_own + 2)
    for k in range(1, zn):
        pieces_end(k)

    p_t, z_s, z_b, z_a = ids(zn), ids(2 * zn), ids(2 * zn), ids(2 * zn)
    side = z // 2
    order = (3 * (1 - side), 2 - side, z + 1 - 2 * (z % 2), z)
    parts = [slice(c * n.rows // 2, (c + 1) * n.rows // 2) for c in range(2)]

    def to_line(i, c, cond_up, cond_down):
        s, here = order[i], parts[c]
        for dst, base, dev, cond in ((zb, z_b, up, cond_up), (za, z_a, down, cond_down)):
            send(zs.at[s, here], dst.at[s, here], z_s + 2 * i + c, base + 2 * s + c, dev, cond)

    def chain(i, c):
        s, here = order[i], parts[c]
        for ref, base, cond in ((zb, z_b, inner & (s > z)), (za, z_a, inner & (s < z))):
            arrive(ref.at[s, here], base + 2 * s + c, cond)

            @pl.when(cond)
            def _():
                zs[s, here] = (acc[i, here] + ref[s, here].astype(f32)).astype(low)

        to_line(i, c, inner & (s > z), inner & (s < z))

    for i, s in enumerate(order):
        def gated(a, here):
            c = conv(a * gsus[0:1, here], ct[0:1, here], ct[1:2, here], ct[2:3, here]) + ct[3:4, here]
            return c / (1.0 + jnp.exp(-c))

        def product(at, width):
            here = pl.ds(at, width)
            return dot(ng[s, 0], gu[:n.half, here]) + dot(ng[s, 1], gu[n.half:, here])

        for j in range(n.full):
            a = product(j * 2 * LANES, 2 * LANES)
            here = slice(j * LANES, (j + 1) * LANES)
            hid[:, here] = (gated(a[:, :LANES], here) * (a[:, LANES:] * gsus[1:2, here])).astype(low)
        a = product(n.full * 2 * LANES, LANES)
        here = slice(n.full * LANES, n.padded)
        last = gated(a, here) * (pltpu.roll(a, LANES // 2, axis=1) * gsus[1:2, here])
        hid[:, n.full * LANES:] = last.astype(low)[:, :n.tail]
        hid_v = hid[...]
        for fl in range(n.per_half):
            ps[i, :, wide(fl)] = dot(hid_v, dw[n.per_half * (1 - t) + fl]).astype(low)
        send(ps.at[i], pr.at[i], p_t + i, p_t + i, pt)
        for fl in range(n.per_half):
            acc[i, :, wide(fl)] = dot(hid_v, dw[n.per_half * t + fl])
        arrive(pr.at[i], p_t + i)
        acc[i] = acc[i] + pr[i].astype(f32)
        if i < zn - 1:
            @pl.when(ends)
            def _():
                zs[s] = acc[i].astype(low)

            for c in range(2):
                to_line(i, c, z == 0, z == zn - 1)
        if i == 2:
            chain(0, 0)
            chain(0, 1)
    for i, c in ((2, 0), (1, 0), (2, 1), (1, 1)):
        chain(i, c)

    for c, here in enumerate(parts):
        for ref, base, cond in ((zb, z_b, can_down), (za, z_a, can_up)):
            arrive(ref.at[z, here], base + 2 * z + c, cond)

            @pl.when(cond)
            def _():
                acc[zn - 1, here] = acc[zn - 1, here] + ref[z, here].astype(f32)

    for fl in range(n.per_half):
        w = wide(fl)
        scaled = acc[zn - 1, :, w] * sc[n.per_half * t + fl][:, n.slots[6]:n.slots[6] + D]
        out[:, w] = (mid[:, w].astype(f32) + scaled).astype(low)

    for c, cond in pending:
        when(cond, c.wait_send)
    assert used[0] <= SEMAPHORES, used[0]


def in_one_kernel(
    n, tokens, mixer_gain, outer_weight, inner_weight, value_weight, outer_scale, inner_scale,
    value_scale, mixer_taps, mixer_project, project_scale, channel_gain, gate_weight, gate_scale,
    up_weight, up_scale, channel_taps, channel_bias, down_weight, down_scale,
):
    f32, zn = jnp.float32, GROUPS
    scales = [v[None, :] for v in (
        outer_scale, inner_scale, value_scale, gate_scale, up_scale, project_scale, down_scale
    )]
    vm, anywhere = pl.BlockSpec(memory_space=pltpu.VMEM), pl.BlockSpec(memory_space=pl.ANY)
    rows, half, features = n.rows, n.half, n.features

    def V(shape, dtype=low):
        return pltpu.VMEM(shape, dtype)

    scratch = [
        V((rows, half)),
        V((3, 2, n.depth, n.chan), f32), V((n.cols, n.depth), f32),
        V((n.depth, zn * n.quarter), f32), V((n.depth, zn * n.quarter), f32), V((zn * n.quarter, n.depth), f32),
        V((features, 3 * n.chan + n.depth)), V((n.depth, 3 * n.chan + n.depth)),
        V((features, n.wide)), V((n.fs, n.quarter, n.depth)),
        V((zn, n.block, n.wide)), V((zn, n.quarter // 2, n.depth)),
        V((1, n.slots[-1]), f32), V((n.fs, 1, n.slots[-1]), f32), V((3, n.chan), f32), V((2, n.padded), f32), V((4, n.padded), f32),
        V((2, rows, LANES), f32), V((2, rows, LANES), f32),
        V((2, 2, rows, half)), V((2, rows, half)), V((2, rows, half)), V((rows, half)), V((rows, half)),
        V((rows, half)), V((zn, 2, rows, half)), V((rows, n.quarter)), V((zn, rows, half), f32),
        V((zn, rows, half)), V((zn, rows, half)), V((zn, rows, half)), V((zn, rows, half)), V((zn, rows, half)),
        pltpu.SemaphoreType.DMA((16,)), pltpu.SemaphoreType.DMA((SEMAPHORES,)), pltpu.SemaphoreType.DMA((SEMAPHORES,)),
    ]
    return pl.pallas_call(
        functools.partial(layer_kernel, n),
        out_shape=jax.ShapeDtypeStruct(tokens.shape, tokens.dtype),
        in_specs=[anywhere] + [vm] * 12 + [anywhere] * 7,
        out_specs=vm,
        scratch_shapes=scratch,
        compiler_params=pltpu.CompilerParams(
            collective_id=0, has_side_effects=True, vmem_limit_bytes=VMEM_BYTES
        ),
    )(
        tokens, mixer_gain[None, :], channel_gain[None, :], mixer_taps, channel_taps, channel_bias[None, :], *scales,
        outer_weight, inner_weight, value_weight, mixer_project, gate_weight, up_weight, down_weight,
    )


def solution(mesh):
    placed = (
        P(("rep", "fs"), "tp"),
        P("tp"),
        P("fs", "tp"),
        P("fs", "tp"),
        P("fs", "tp"),
        P(("tp", "fs")),
        P(("tp", "fs")),
        P(("tp", "fs")),
        P(None, "tp"),
        P("tp", "fs"),
        P("fs"),
        P("tp"),
        P("fs", "tp"),
        P(("tp", "fs")),
        P("fs", "tp"),
        P(("tp", "fs")),
        P(None, "tp"),
        P("tp"),
        P("tp", "fs"),
        P("fs"),
    )
    return jax.shard_map(
        per_device, mesh=mesh, in_specs=placed, out_specs=P(("rep", "fs"), "tp"), check_vma=False
    )
```

```python
import functools

import jax
import jax.numpy as jnp
from jax import lax
from jax.experimental import pallas as pl
from jax.experimental.pallas import tpu as pltpu
from jax.sharding import PartitionSpec as P

LEN = 320
GROUPS = 4
LANES = 128
SEMAPHORES = 256
VMEM_BYTES = 65000 * 1024
MESH = pl.DeviceIdType.MESH

epsilon = 1e-06
low = jnp.bfloat16


class Place:
    def __init__(self):
        self.fs = lax.axis_size("fs")
        self.reps = lax.axis_size("rep")
        self.tps = lax.axis_size("tp")
        self.slow = GROUPS if self.fs % GROUPS == 0 else 1
        self.fast = self.fs // self.slow
        at = lax.axis_index("fs")
        self.z, self.y = at // self.fast, at % self.fast
        self.r, self.t = lax.axis_index("rep"), lax.axis_index("tp")

    def from_slow(self, block, shift):
        perm = [(z * self.fast + y, (z - shift) % self.slow * self.fast + y)
                for z in range(self.slow) for y in range(self.fast)]
        return lax.ppermute(block, "fs", perm)

    def from_fast(self, block, shift):
        perm = [(z * self.fast + y, z * self.fast + (y - shift) % self.fast)
                for z in range(self.slow) for y in range(self.fast)]
        return lax.ppermute(block, "fs", perm)

    def from_rep(self, block, shift):
        return lax.ppermute(block, "rep", [(i, (i - shift) % self.reps) for i in range(self.reps)])

    def from_tp(self, block, shift):
        return lax.ppermute(block, "tp", [(i, (i - shift) % self.tps) for i in range(self.tps)])

    def spread(self, pieces, axis):
        held = jnp.concatenate(pieces, axis)
        held = jnp.concatenate([held] + [self.from_fast(held, j) for j in range(1, self.fast)], axis)
        return jnp.concatenate([held] + [self.from_rep(held, i) for i in range(1, self.reps)], axis)

    def order(self, width):
        return [
            (((self.z + k) % self.slow * self.fast + (self.y + j) % self.fast) * self.reps
             + (self.r + i) % self.reps) * width
            for i in range(self.reps) for j in range(self.fast) for k in range(self.slow)
        ]

    def position(self, block):
        f, part = block // self.reps, block % self.reps
        i = (part - self.r) % self.reps
        j = (f % self.fast - self.y) % self.fast
        k = (f // self.fast - self.z) % self.slow
        return (i * self.fast + j) * self.slow + k


def columns(values, offsets, width):
    return jnp.concatenate(
        [lax.dynamic_slice(values, (0, offset), (values.shape[0], width)) for offset in offsets], axis=1
    )


def inverse_norm(place, values):
    own = jnp.sum(values * values, axis=1)
    total = own
    for s in range(1, place.tps):
        total = total + place.from_tp(own, s)
    return lax.rsqrt(total / (values.shape[1] * place.tps) + epsilon)


def normalize(place, token_rows, gain):
    values = token_rows.astype(jnp.float32)
    return (values * inverse_norm(place, values)[:, None] * gain).astype(low)


def all_features(place, local, width):
    held = jnp.concatenate([local] + [place.from_tp(local, s) for s in range(1, place.tps)], axis=1)
    whole = held.shape[1]
    offsets = [(offset - place.t * local.shape[1]) % whole for offset in place.order(width)]
    return columns(held, offsets, width)


def own_features(place, product, width):
    local = product.shape[1] // place.tps
    count = local // width

    def share(peer):
        return columns(product, [place.position(peer * count + b) * width for b in range(count)], width)

    total = share(place.t)
    for s in range(1, place.tps):
        total = total + place.from_tp(share((place.t - s) % place.tps).astype(low), s).astype(jnp.float32)
    return total


def causal_taps(values, taps):
    tap_count = taps.shape[0]
    grouped = values.reshape(-1, LEN, values.shape[1])
    padded = jnp.pad(grouped, ((0, 0), (tap_count - 1, 0), (0, 0)))
    running = jnp.zeros_like(grouped)
    for offset in range(tap_count):
        running = running + taps[offset] * padded[:, offset : offset + LEN]
    return running.reshape(values.shape)


def dot(left, right):
    return jnp.dot(left, right, preferred_element_type=jnp.float32)


def per_device(
    tokens, mixer_gain, outer_weight, inner_weight, value_weight, outer_scale, inner_scale,
    value_scale, mixer_taps, mixer_project, project_scale, channel_gain, gate_weight, gate_scale,
    up_weight, up_scale, channel_taps, channel_bias, down_weight, down_scale,
):
    sizes = Sizes(
        tuple(lax.axis_size(a) for a in ("rep", "fs", "tp")), tokens, outer_weight, gate_weight, mixer_project
    )
    if sizes.fits(mixer_project):
        return in_one_kernel(
            sizes, tokens, mixer_gain, outer_weight, inner_weight, value_weight, outer_scale, inner_scale,
            value_scale, mixer_taps, mixer_project, project_scale, channel_gain, gate_weight, gate_scale,
            up_weight, up_scale, channel_taps, channel_bias, down_weight, down_scale,
        )
    place = Place()
    rows = outer_weight.shape[0] // place.reps
    width = mixer_project.shape[1] // place.reps
    slow = place.slow
    quarter = gate_weight.shape[1] // slow

    def row_share(weight):
        return lax.dynamic_slice_in_dim(weight, place.r * rows, rows, 0).astype(low)

    def column_share(weight):
        return lax.dynamic_slice_in_dim(weight, place.r * width, width, 1).astype(low)

    def same(piece):
        return [piece] + [place.from_slow(piece, k) for k in range(1, slow)]

    def exchange(take):
        return [take(place.z)] + [
            place.from_slow(take((place.z - k) % slow), k) for k in range(1, slow)
        ]

    mixer_in = place.spread(
        same(jnp.concatenate([row_share(w) for w in (outer_weight, inner_weight, value_weight)], axis=1)), 0
    )
    project = place.spread(same(column_share(mixer_project)), 1)

    def column_part(weight):
        parts = row_share(weight).reshape(rows, slow, quarter).transpose(1, 0, 2)
        return lambda z: lax.dynamic_index_in_dim(parts, z, 0, keepdims=False)

    gate_full = place.spread(exchange(column_part(gate_weight)), 0)
    up_full = place.spread(exchange(column_part(up_weight)), 0)
    down_share = column_share(down_weight)
    down_full = place.spread(
        exchange(lambda z: lax.dynamic_slice_in_dim(down_share, z * quarter, quarter, 0)), 1
    )

    scales = (outer_scale, inner_scale, value_scale, gate_scale, up_scale, project_scale, down_scale)
    packed = lax.all_gather(jnp.concatenate(scales), "fs", axis=0)
    ends, full = 0, []
    for scale in scales:
        full.append(packed[:, ends : ends + scale.shape[0]].reshape(-1))
        ends += scale.shape[0]
    outer_all, inner_all, value_all, gate_all, up_all, project_all, down_all = full
    local = tokens.shape[1]

    def mine(vector, at, size):
        return lax.dynamic_slice_in_dim(vector, at * size, size, vector.ndim - 1)

    normed = all_features(place, normalize(place, tokens, mixer_gain), rows)
    parts = dot(normed, mixer_in)
    each = outer_weight.shape[1]
    outer_part = parts[:, :each] * outer_all
    conv_input = parts[:, each : 2 * each] * inner_all * (parts[:, 2 * each :] * value_all)
    mixed = (outer_part * causal_taps(conv_input, mixer_taps)).astype(low)
    mixer_sum = own_features(place, dot(mixed, project), width) * mine(project_all, place.t, local)
    middle = (tokens.astype(jnp.float32) + mixer_sum).astype(low)

    normed_own = normalize(place, middle, channel_gain)
    normed_two = jnp.concatenate(
        [normed_own] + [place.from_slow(normed_own, k) for k in range(1, slow)], axis=0
    )
    normed_two = all_features(place, normed_two, rows)
    gate_part = dot(normed_two, gate_full) * mine(gate_all, place.z, quarter)
    up_part = dot(normed_two, up_full) * mine(up_all, place.z, quarter)
    hidden = (
        jax.nn.silu(
            causal_taps(gate_part, mine(channel_taps, place.z, quarter))
            + mine(channel_bias, place.z, quarter)
        )
        * up_part
    ).astype(low)
    share = own_features(place, dot(hidden, down_full), width)
    count = tokens.shape[0]
    total = share[:count]
    for k in range(1, slow):
        sent = share[k * count : (k + 1) * count].astype(low)
        total = total + place.from_slow(sent, -k).astype(jnp.float32)
    return (middle.astype(jnp.float32) + total * mine(down_all, place.t, local)).astype(low)


class Sizes:
    def __init__(self, mesh_sizes, tokens, outer_weight, gate_weight, mixer_project):
        self.reps, self.fs, self.tps = mesh_sizes
        self.rows, self.half = tokens.shape
        self.depth, self.cols = outer_weight.shape
        self.block = self.depth // 2
        self.chan = self.cols // 2
        self.quarter = gate_weight.shape[1] // GROUPS
        self.full = self.quarter // LANES
        self.tail = self.quarter % LANES
        self.padded = (self.full + 1) * LANES
        self.wide = 2 * self.quarter
        self.per_half = self.fs // 2
        self.features = self.half * self.tps
        each = self.chan // self.per_half
        self.slots = [0]
        for width in [each] * 3 + [self.quarter // 2] * 2 + [self.depth] * 2:
            self.slots.append(self.slots[-1] + -(-width // LANES) * LANES)
        self.halves = 2 * each == LANES and 2 * (self.slots[4] - self.slots[3]) == self.padded

    def fits(self, mixer_project):
        return (
            (self.reps, self.fs, self.tps) == (2, 2 * GROUPS, 2)
            and self.rows == LEN
            and self.depth % (2 * LANES) == 0
            and self.per_half * self.depth == self.half
            and self.cols == 4 * self.block
            and self.halves
            and self.tail == LANES // 2
            and self.quarter % 32 == 0
            and mixer_project.shape[1] == self.depth
        )


def layer_kernel(
    n, tok_h, mg, cg, mt, channel_taps, channel_bias, s_o, s_i, s_v, s_g, s_u, s_p, s_d,
    ow, iw, vw, pw, gw, uw, dn, out,
    tok, st_m, st_p, st_g, st_u, st_d, mw, ms, gu, dw, sg, sd, pk, sc, msc, gsus, ct, sq, sqr,
    xg, mps, mpr, ys, yr, mid, ng, hid, acc, ps, pr, zs, zb, za, lsem, ss, rs,
):
    f32 = jnp.float32
    zn = GROUPS
    r, f, t = lax.axis_index("rep"), lax.axis_index("fs"), lax.axis_index("tp")
    z, y = f // 2, f % 2
    py, px, pt = (r, f + 1 - 2 * y, t), (1 - r, f, t), (r, f, 1 - t)
    fy = 2 * z + 1 - y
    up, down = (r, (f + 2) % n.fs, t), (r, (f + n.fs - 2) % n.fs, t)
    can_up, can_down = z < zn - 1, z > 0
    inner = (z > 0) & (z < zn - 1)
    ends = (z == 0) | (z == zn - 1)
    D, B, CH, Q = n.depth, n.block, n.chan, n.quarter

    used = [0]
    pending = []

    def ids(count=1):
        used[0] += count
        return used[0] - count

    def when(cond, fn):
        if cond is None:
            fn()
        else:
            pl.when(cond)(fn)

    def send(src, dst, sid, rid, dev, cond=None):
        c = pltpu.make_async_remote_copy(
            src_ref=src, dst_ref=dst, send_sem=ss.at[sid], recv_sem=rs.at[rid],
            device_id=dev, device_id_type=MESH,
        )
        when(cond, c.start)
        pending.append((c, cond))

    def arrive(dst, rid, cond=None):
        c = pltpu.make_async_remote_copy(
            src_ref=dst, dst_ref=dst, send_sem=ss.at[0], recv_sem=rs.at[rid],
            device_id=pt, device_id_type=MESH,
        )
        when(cond, c.wait_recv)

    def place(fb, rh):
        return pl.multiple_of((fb // n.per_half) * n.half + rh * (n.half // 2) + (fb % n.per_half) * B, B)

    def dot(a, b):
        return jnp.dot(a, b, preferred_element_type=f32)

    def conv(v, w0, w1, w2):
        at = lax.broadcasted_iota(jnp.int32, v.shape, 0)
        one = jnp.where(at >= 1, pltpu.roll(v, 1, axis=0), 0.0)
        two = jnp.where(at >= 2, pltpu.roll(v, 2, axis=0), 0.0)
        return w0 * two + w1 * one + w2 * v

    loads = []

    def load(src, dst):
        c = pltpu.make_async_copy(src, dst, lsem.at[len(loads)])
        c.start()
        loads.append(c)
        return c

    load_tok = load(tok_h, tok)
    load_m = []
    for m, w in enumerate((ow, iw, vw)):
        for h in range(2):
            load_m.append(load(w.at[:, h * CH:(h + 1) * CH], st_m.at[m, h]))
    load_m.append(load(pw, st_p))
    load_f = [load(gw, st_g), load(uw, st_u), load(dn, st_d)]

    barrier = pltpu.get_barrier_semaphore()
    for k in range(1, n.fs):
        pl.semaphore_signal(barrier, inc=1, device_id=(r, (f + k) % n.fs, t), device_id_type=MESH)
    pl.semaphore_signal(barrier, inc=1, device_id=px, device_id_type=MESH)
    pl.semaphore_signal(barrier, inc=1, device_id=pt, device_id_type=MESH)

    for c in load_m:
        c.wait()
    for rh in range(2):
        here = slice(rh * B, (rh + 1) * B)
        for m in range(3):
            ms[here, m * CH:(m + 1) * CH] = st_m[m, 1 - y, here, :].astype(low)
            mw[pl.ds(place(f, rh), B), m * CH:(m + 1) * CH] = st_m[m, y, here, :].astype(low)
        for h, ref, rows in ((1 - y, ms, here), (y, mw, pl.ds(place(f, rh), B))):
            ref[rows, 3 * CH:] = st_p[pl.ds(pl.multiple_of(h * CH + rh * B, B), B), :].astype(low)

    pk[...] = jnp.zeros_like(pk)
    for at, ref in zip(n.slots, (s_o, s_i, s_v, s_g, s_u, s_p, s_d)):
        pk[:, at:at + ref.shape[0]] = ref[...][None, :]
    for q in range(zn):
        @pl.when(z == q)
        def _():
            base = q * Q // LANES * LANES
            for ref, rows in ((channel_taps, slice(0, 3)), (channel_bias, slice(3, 4))):
                taps = ref[:, base:base + n.padded] if len(ref.shape) == 2 else ref[base:base + n.padded][None, :]
                ct[rows, :] = pltpu.roll(taps, n.padded - LANES // 2, axis=1) if q * Q % LANES else taps

    load_tok.wait()

    def square_sum(values):
        return jnp.sum(values * values, axis=1, keepdims=True)

    sq_id = ids(2)

    def share_squares(which, total):
        sq[which] = jnp.broadcast_to(total, (n.rows, LANES))
        send(sq.at[which], sqr.at[which], sq_id + which, sq_id + which, pt)

    own_squares = square_sum(tok[...].astype(f32))
    pl.semaphore_wait(barrier, n.fs + 1)
    share_squares(0, own_squares)

    m1 = ids(2)

    def block_at(fb, rh):
        return mw.at[pl.ds(place(fb, rh), B)]

    def send_m1(rh):
        send(ms.at[pl.ds(pl.multiple_of(rh * B, B), B)], block_at(f, rh), m1 + rh, m1 + rh, py)

    def arrive_m1(rh):
        arrive(block_at(fy, rh), m1 + rh)

    send_m1(r)

    class Line:
        def __init__(self, block):
            self.block = block
            self.up, self.down, self.below, self.above = ids(zn), ids(zn), ids(zn), ids(zn)

        def forward(self, at, k, upward, cond):
            b = self.block(at)
            send(b, b, (self.up if upward else self.down) + k, (self.below if upward else self.above) + k + 1,
                 up if upward else down, cond)

        def start(self):
            self.forward(z, 0, True, can_up)
            self.forward(z, 0, False, can_down)

        def step(self, k, then):
            a, b = (z + zn - k) % zn, (z + k) % zn
            for at, base, upward, cond, more in (
                (a, self.below, True, z >= k, can_up), (b, self.above, False, z < zn - k, can_down),
            ):
                arrive(self.block(at), base + k, cond)
                if k < zn - 1:
                    self.forward(at, k, upward, cond & more)
                then(at, k, upward, cond)

    own_line = Line(lambda at: block_at(2 * at + y, r))
    other_line = Line(lambda at: block_at(2 * at + 1 - y, r))
    own_line.start()

    def inverse_norm_of(which, own):
        arrive(sqr.at[which], sq_id + which)
        return lax.rsqrt((own + sqr[which][:, :1]) / n.features + epsilon)

    def normalize(values, rows, inverse, gain, dst):
        for fl in range(n.per_half):
            for rh in range(2):
                here = slice((2 * fl + rh) * B, (2 * fl + rh + 1) * B)
                there = slice((rh * n.per_half + fl) * B, (rh * n.per_half + fl + 1) * B)
                dst[rows, there] = (values[rows, here].astype(f32) * inverse[rows] * gain[:, here]).astype(low)

    whole = slice(0, n.rows)
    parts = [slice(c * n.rows // 2, (c + 1) * n.rows // 2) for c in range(2)]

    normalize(tok, whole, inverse_norm_of(0, own_squares), mg, xg.at[y, t])
    x_y, x_t = ids(), ids(2)
    send(xg.at[y, t], xg.at[y, t], x_y, x_y, py)
    send(xg.at[y, t], xg.at[y, t], x_t, x_t, pt)
    send_m1(1 - r)

    scale_s, scale_r = ids(n.fs), ids(n.fs)
    sc[f] = pk[...]
    for k in range(1, n.fs):
        send(pk, sc.at[f], scale_s + k, scale_r + f, (r, (f + k) % n.fs, t))

    mx = ids(4 * zn)

    def over_x(which, blk):
        def then(at, k, upward, cond):
            s = mx + 4 * k + 2 * which + (1 if upward else 0)
            send(blk(at), blk(at), s, s, px, cond)
        return then

    for c in load_f:
        c.wait()

    def tiles(rows, q):
        base = q * Q // LANES * LANES
        g = st_g[rows, base:base + n.padded]
        u = st_u[rows, base:base + n.padded]
        if q * Q % LANES:
            g = pltpu.roll(g, n.padded - LANES // 2, axis=1)
            u = pltpu.roll(u, n.padded - LANES // 2, axis=1)
        parts = []
        for j in range(n.full):
            parts += [g[:, j * LANES:(j + 1) * LANES], u[:, j * LANES:(j + 1) * LANES]]
        lane = lax.broadcasted_iota(jnp.int32, (B, LANES), 1)
        parts.append(jnp.where(lane < LANES // 2, g[:, n.full * LANES:], pltpu.roll(u[:, n.full * LANES:], LANES // 2, axis=1)))
        return parts

    for q in range(zn):
        @pl.when(z == q)
        def _():
            for rh in range(2):
                for j, piece in enumerate(tiles(pl.ds(rh * B, B), q)):
                    gu[pl.ds(place(f, rh), B), j * LANES:(j + 1) * LANES] = piece.astype(low)

        @pl.when(z != q)
        def _():
            for j, piece in enumerate(tiles(pl.ds(pl.multiple_of(r * B, B), B), q)):
                sg[q, :, j * LANES:(j + 1) * LANES] = piece.astype(low)

        sd[q] = st_d[pl.ds(pl.multiple_of(q * Q + r * (Q // 2), 16), Q // 2), :].astype(low)
    dw[f] = st_d[pl.ds(pl.multiple_of(z * Q, 16), Q), :].astype(low)

    def gu_at(fb, rh):
        return gu.at[pl.ds(place(fb, rh), B)]

    def dw_at(fb, rh):
        return dw.at[fb, pl.ds(pl.multiple_of(rh * (Q // 2), 16), Q // 2)]

    fy_own = ids(4)
    for rh in range(2):
        send(gu_at(f, rh), gu_at(f, rh), fy_own + rh, fy_own + rh, py)
    send(dw_at(f, r), dw_at(f, r), fy_own + 2, fy_own + 2, py)

    f1, f2y, f2x, f2d = ids(2 * zn), ids(2 * zn), ids(2 * zn), ids(2 * zn)

    def across(k):
        if k == 1:
            return z + 1 - 2 * (z % 2)
        if k == 2:
            return z + 2 - 4 * (z // 2)
        return zn - 1 - z

    def stage_one(k, cond):
        q = across(k)
        dev = (r, 2 * q + y, t)
        send(sg.at[q], gu_at(f, r), f1 + 2 * k, f1 + 2 * k, dev, cond)
        send(sd.at[q], dw_at(f, r), f1 + 2 * k + 1, f1 + 2 * k + 1, dev, cond)

    def held(k):
        fb = 2 * across(k) + y
        return enumerate((gu_at(fb, r), dw_at(fb, r)))

    def pieces_over_x(k, cond):
        for i, ref in held(k):
            arrive(ref, f1 + 2 * k + i, cond)
            send(ref, ref, f2x + 2 * k + i, f2x + 2 * k + i, px, cond)

    def pieces_over_y(k):
        for i, ref in held(k):
            send(ref, ref, f2y + 2 * k + i, f2y + 2 * k + i, py)

    def pieces_on(k):
        gates = gu_at(2 * across(k) + 1 - y, r)
        arrive(gates, f2y + 2 * k)
        send(gates, gates, f2d + 2 * k, f2d + 2 * k, px)
        downs = dw_at(2 * across(k) + y, 1 - r)
        arrive(downs, f2x + 2 * k + 1)
        send(downs, downs, f2d + 2 * k + 1, f2d + 2 * k + 1, py)

    def gates_end(k):
        arrive(gu_at(2 * across(k) + y, 1 - r), f2x + 2 * k)
        arrive(gu_at(2 * across(k) + 1 - y, 1 - r), f2d + 2 * k)

    def downs_end(k):
        arrive(dw_at(2 * across(k) + 1 - y, r), f2y + 2 * k + 1)
        arrive(dw_at(2 * across(k) + 1 - y, 1 - r), f2d + 2 * k + 1)

    arrive_m1(r)
    other_line.start()
    stage_one(1, ends)
    own_x, other_x = over_x(0, own_line.block), over_x(1, other_line.block)
    own_line.step(1, own_x)
    other_line.step(1, other_x)
    own_line.step(2, own_x)
    arrive(xg.at[1 - y, t], x_y)
    send(xg.at[1 - y, t], xg.at[1 - y, t], x_t + 1, x_t + 1, pt)
    other_line.step(2, other_x)
    stage_one(2, ends)
    stage_one(3, inner)
    own_line.step(3, own_x)
    other_line.step(3, other_x)

    for k in range(1, n.fs):
        fk = (f + k) % n.fs
        arrive(sc.at[fk], scale_r + fk)
    for m, at in enumerate(n.slots[:3]):
        slot = slice(at, at + LANES)
        for j in range(CH // LANES):
            fb = n.per_half * y + 2 * j
            msc[m:m + 1, j * LANES:(j + 1) * LANES] = sc[fb][:, slot] + pltpu.roll(sc[fb + 1][:, slot], LANES // 2, axis=1)
    for i, at in enumerate(n.slots[3:5]):
        first, second = (
            jnp.concatenate([sc[2 * z + h][:, at:at + n.padded // 2], jnp.zeros((1, n.padded // 2), f32)], axis=1)
            for h in range(2)
        )
        gsus[i:i + 1, :] = first + pltpu.roll(second, Q // 2, axis=1)
    arrive_m1(1 - r)
    for i in range(2):
        arrive(xg.at[y if i == 0 else 1 - y, 1 - t], x_t + i)
    near = z // 2

    def arrive_mixer(k, own_half, streams=(0, 1)):
        for side, at, cond in ((1, (z + zn - k) % zn, z >= k), (0, (z + k) % zn, z < zn - k)):
            for which in streams:
                fb = 2 * at + (1 - y if which else y)
                same = at // 2 == near
                arrive(block_at(fb, 1 - r), mx + 4 * k + 2 * which + side, cond & (same if own_half else ~same))

    arrive_mixer(1, True)
    near_rows = pl.ds(pl.multiple_of(near * n.half, n.half), n.half)
    far_rows = pl.ds(pl.multiple_of((1 - near) * n.half, n.half), n.half)
    for i, sy in enumerate((1 - y, y)):
        for m in range(3):
            here = slice(m * CH, (m + 1) * CH)
            acc[2 + i, :, here] = dot(xg[sy, near], mw[near_rows, here])
    arrive_mixer(1, False)
    stage_one(1, inner)
    arrive_mixer(2, False)
    arrive_mixer(3, False)

    y_lanes = pl.ds(pl.multiple_of(y * CH, CH), CH)
    m_taps = [mt[k:k + 1, y_lanes] for k in range(3)]
    mt_id, my_id = ids(3), ids(2)
    pad = 16

    def wide(fl):
        return slice(fl * D, (fl + 1) * D)

    def with_past(rows):
        first = max(rows.start - pad, 0)
        return slice(first, rows.stop), rows.start - first

    def mix(i, rows, at):
        sy = (1 - y, y)[i]
        long, drop = with_past(rows)

        def part(m):
            here = slice(m * CH, (m + 1) * CH)
            return (acc[2 + i, long, here] + dot(xg[sy, 1 - near, long], mw[far_rows, here])) * msc[m:m + 1, :]

        cv = conv(part(1) * part(2), *m_taps)
        mixed = (part(0) * cv).astype(low)[drop:]

        def project(fb):
            return dot(mixed, jnp.concatenate([mw[pl.ds(place(fb, rh), B), 3 * CH:] for rh in range(2)], axis=0))

        for fl in range(n.per_half):
            mps[i, rows, wide(fl)] = project(n.per_half * (1 - t) + fl).astype(low)
        send(mps.at[i, rows], mpr.at[i, rows], mt_id + at, mt_id + at, pt)
        for fl in range(n.per_half):
            acc[i, rows, wide(fl)] = project(n.per_half * t + fl)

    for c, rows in enumerate(parts):
        mix(0, rows, c)
        arrive(mpr.at[0, rows], mt_id + c)
        ys[rows] = (acc[0, rows] + mpr[0, rows].astype(f32)).astype(low)
        send(ys.at[rows], yr.at[rows], my_id + c, my_id + c, py)
    stage_one(2, inner)
    arrive(dw_at(fy, r), fy_own + 2)
    send(dw_at(fy, r), dw_at(fy, r), fy_own + 3, fy_own + 3, px)
    pieces_over_x(1, None)
    mix(1, whole, 2)
    arrive(mpr.at[1], mt_id + 2)

    pieces_over_x(3, inner)
    pieces_over_x(2, inner)

    pieces_over_y(1)
    arrive(yr.at[parts[0]], my_id)
    stage_one(3, ends)
    arrive(yr.at[parts[1]], my_id + 1)
    total_sq = None
    for fl in range(n.per_half):
        w = wide(fl)
        added = (acc[1, :, w] + mpr[1, :, w].astype(f32) + yr[:, w].astype(f32)) * sc[n.per_half * t + fl][:, n.slots[5]:n.slots[5] + D]
        middle = (tok[:, w].astype(f32) + added).astype(low)
        mid[:, w] = middle
        part_sq = square_sum(middle.astype(f32))
        total_sq = part_sq if total_sq is None else total_sq + part_sq
    share_squares(1, total_sq)
    inverse = inverse_norm_of(1, total_sq)

    n_t = ids(4 * zn)
    token_lines = []
    for c, rows in enumerate(parts):
        normalize(mid, rows, inverse, cg, ng.at[z, t])
        line = Line(lambda at, rows=rows: ng.at[at, t, rows])
        line.start()
        token_lines.append(line)
        send(line.block(z), line.block(z), n_t + c, n_t + c, pt)

    def token_step(k):
        for c, line in enumerate(token_lines):
            def to_core(at, k, upward, cond):
                s = n_t + 4 * k + (2 if upward else 0) + c
                send(line.block(at), line.block(at), s, s, pt, cond)

            line.step(k, to_core)

    for k in (2, 3):
        pieces_over_x(k, ends)
        pieces_over_y(k)
    pieces_on(1)
    token_step(1)
    pieces_on(2)
    pieces_on(3)
    token_step(2)
    def core_step(k):
        for c, rows in enumerate(parts):
            for side, at, cond in ((2, (z + zn - k) % zn, z >= k), (0, (z + k) % zn, z < zn - k)):
                arrive(ng.at[at, 1 - t, rows], n_t + 4 * k + side + c, cond)

    for c, rows in enumerate(parts):
        arrive(ng.at[z, 1 - t, rows], n_t + c)
    core_step(1)
    core_step(2)
    for rh in range(2):
        arrive(gu_at(fy, rh), fy_own + rh)
    for k in range(1, zn):
        gates_end(k)

    p_t, z_s, z_b, z_a = ids(6), ids(2 * zn), ids(2 * zn), ids(2 * zn)
    side = z // 2
    order = (2 - side, 3 * (1 - side), z + 1 - 2 * (z % 2), z)

    def to_line(i, c, cond_up, cond_down):
        s, here = order[i], parts[c]
        for dst, base, dev, cond in ((zb, z_b, up, cond_up), (za, z_a, down, cond_down)):
            send(zs.at[s, here], dst.at[s, here], z_s + 2 * i + c, base + 2 * s + c, dev, cond)

    def chain(i, c):
        s, here = order[i], parts[c]
        for ref, base, cond in ((zb, z_b, inner & (s > z)), (za, z_a, inner & (s < z))):
            arrive(ref.at[s, here], base + 2 * s + c, cond)

            @pl.when(cond)
            def _():
                zs[s, here] = (acc[i, here] + ref[s, here].astype(f32)).astype(low)

        to_line(i, c, inner & (s > z), inner & (s < z))

    def gated(a, here):
        c = conv(a * gsus[0:1, here], ct[0:1, here], ct[1:2, here], ct[2:3, here]) + ct[3:4, here]
        return c / (1.0 + jnp.exp(-c))

    def hidden(s, rows):
        long, drop = with_past(rows)

        def product(at, width):
            here = slice(at, at + width)
            return dot(ng[s, 0, long], gu[:n.half, here]) + dot(ng[s, 1, long], gu[n.half:, here])

        for j in range(n.full):
            a = product(j * 2 * LANES, 2 * LANES)
            here = slice(j * LANES, (j + 1) * LANES)
            hid[rows, here] = (gated(a[:, :LANES], here) * (a[:, LANES:] * gsus[1:2, here])).astype(low)[drop:]
        a = product(n.full * 2 * LANES, LANES)
        here = slice(n.full * LANES, n.padded)
        last = gated(a, here) * (pltpu.roll(a, LANES // 2, axis=1) * gsus[1:2, here])
        hid[rows, n.full * LANES:] = last.astype(low)[drop:, :n.tail]

    def back(i, rows, at):
        hid_v = hid[rows]
        for fl in range(n.per_half):
            ps[i, rows, wide(fl)] = dot(hid_v, dw[n.per_half * (1 - t) + fl]).astype(low)
        send(ps.at[i, rows], pr.at[i, rows], p_t + at, p_t + at, pt)
        for fl in range(n.per_half):
            acc[i, rows, wide(fl)] = dot(hid_v, dw[n.per_half * t + fl])
        arrive(pr.at[i, rows], p_t + at)
        acc[i, rows] = acc[i, rows] + pr[i, rows].astype(f32)
        if i < zn - 1:
            @pl.when(ends)
            def _():
                zs[order[i], rows] = acc[i, rows].astype(low)

    def outward(i, c):
        to_line(i, c, z == 0, z == zn - 1)

    hidden(order[0], parts[0])
    arrive(dw_at(fy, 1 - r), fy_own + 3)
    for k in range(1, zn):
        downs_end(k)
    back(0, parts[0], 0)
    outward(0, 0)
    hidden(order[0], parts[1])
    back(0, parts[1], 1)
    token_step(3)
    core_step(3)
    for c in range(2):
        hidden(order[1], parts[c])
        back(1, parts[c], 2 + c)
        outward(1, c)
    outward(0, 1)
    hidden(order[2], whole)
    back(2, whole, 4)
    outward(2, 0)
    outward(2, 1)
    chain(0, 0)
    chain(1, 0)
    hidden(order[3], whole)
    back(3, whole, 5)
    for i, c in ((1, 1), (2, 0), (0, 1), (2, 1)):
        chain(i, c)

    for c, here in enumerate(parts):
        for ref, base, cond in ((zb, z_b, can_down), (za, z_a, can_up)):
            arrive(ref.at[z, here], base + 2 * z + c, cond)

            @pl.when(cond)
            def _():
                acc[zn - 1, here] = acc[zn - 1, here] + ref[z, here].astype(f32)

    for fl in range(n.per_half):
        w = wide(fl)
        scaled = acc[zn - 1, :, w] * sc[n.per_half * t + fl][:, n.slots[6]:n.slots[6] + D]
        out[:, w] = (mid[:, w].astype(f32) + scaled).astype(low)

    for c, cond in pending:
        when(cond, c.wait_send)
    assert used[0] <= SEMAPHORES, used[0]


def in_one_kernel(
    n, tokens, mixer_gain, outer_weight, inner_weight, value_weight, outer_scale, inner_scale,
    value_scale, mixer_taps, mixer_project, project_scale, channel_gain, gate_weight, gate_scale,
    up_weight, up_scale, channel_taps, channel_bias, down_weight, down_scale,
):
    f32, zn = jnp.float32, GROUPS
    scales = (outer_scale, inner_scale, value_scale, gate_scale, up_scale, project_scale, down_scale)
    vm, anywhere = pl.BlockSpec(memory_space=pltpu.VMEM), pl.BlockSpec(memory_space=pl.ANY)
    rows, half, features = n.rows, n.half, n.features

    def V(shape, dtype=low):
        return pltpu.VMEM(shape, dtype)

    scratch = [
        V((rows, half)),
        V((3, 2, n.depth, n.chan), f32), V((n.cols, n.depth), f32),
        V((n.depth, zn * n.quarter), f32), V((n.depth, zn * n.quarter), f32), V((zn * n.quarter, n.depth), f32),
        V((features, 3 * n.chan + n.depth)), V((n.depth, 3 * n.chan + n.depth)),
        V((features, n.wide)), V((n.fs, n.quarter, n.depth)),
        V((zn, n.block, n.wide)), V((zn, n.quarter // 2, n.depth)),
        V((1, n.slots[-1]), f32), V((n.fs, 1, n.slots[-1]), f32), V((3, n.chan), f32), V((2, n.padded), f32), V((4, n.padded), f32),
        V((2, rows, LANES), f32), V((2, rows, LANES), f32),
        V((2, 2, rows, half)), V((2, rows, half)), V((2, rows, half)), V((rows, half)), V((rows, half)),
        V((rows, half)), V((zn, 2, rows, half)), V((rows, n.quarter)), V((zn, rows, half), f32),
        V((zn, rows, half)), V((zn, rows, half)), V((zn, rows, half)), V((zn, rows, half)), V((zn, rows, half)),
        pltpu.SemaphoreType.DMA((16,)), pltpu.SemaphoreType.DMA((SEMAPHORES,)), pltpu.SemaphoreType.DMA((SEMAPHORES,)),
    ]
    return pl.pallas_call(
        functools.partial(layer_kernel, n),
        out_shape=jax.ShapeDtypeStruct(tokens.shape, tokens.dtype),
        in_specs=[anywhere] + [vm] * 12 + [anywhere] * 7,
        out_specs=vm,
        scratch_shapes=scratch,
        compiler_params=pltpu.CompilerParams(
            collective_id=0, has_side_effects=True, vmem_limit_bytes=VMEM_BYTES
        ),
    )(
        tokens, mixer_gain[None, :], channel_gain[None, :], mixer_taps, channel_taps, channel_bias, *scales,
        outer_weight, inner_weight, value_weight, mixer_project, gate_weight, up_weight, down_weight,
    )


def solution(mesh):
    placed = (
        P(("rep", "fs"), "tp"),
        P("tp"),
        P("fs", "tp"),
        P("fs", "tp"),
        P("fs", "tp"),
        P(("tp", "fs")),
        P(("tp", "fs")),
        P(("tp", "fs")),
        P(None, "tp"),
        P("tp", "fs"),
        P("fs"),
        P("tp"),
        P("fs", "tp"),
        P(("tp", "fs")),
        P("fs", "tp"),
        P(("tp", "fs")),
        P(None, "tp"),
        P("tp"),
        P("tp", "fs"),
        P("fs"),
    )
    return jax.shard_map(
        per_device, mesh=mesh, in_specs=placed, out_specs=P(("rep", "fs"), "tp"), check_vma=False
    )
```

```python
import functools

import jax
import jax.numpy as jnp
from jax import lax
from jax.experimental import pallas as pl
from jax.experimental.pallas import tpu as pltpu
from jax.sharding import PartitionSpec as P

LEN = 320
GROUPS = 4
LANES = 128
SEMAPHORES = 256
VMEM_BYTES = 65000 * 1024
MESH = pl.DeviceIdType.MESH

epsilon = 1e-06
low = jnp.bfloat16


class Place:
    def __init__(self):
        self.fs = lax.axis_size("fs")
        self.reps = lax.axis_size("rep")
        self.tps = lax.axis_size("tp")
        self.slow = GROUPS if self.fs % GROUPS == 0 else 1
        self.fast = self.fs // self.slow
        at = lax.axis_index("fs")
        self.z, self.y = at // self.fast, at % self.fast
        self.r, self.t = lax.axis_index("rep"), lax.axis_index("tp")

    def from_slow(self, block, shift):
        perm = [(z * self.fast + y, (z - shift) % self.slow * self.fast + y)
                for z in range(self.slow) for y in range(self.fast)]
        return lax.ppermute(block, "fs", perm)

    def from_fast(self, block, shift):
        perm = [(z * self.fast + y, z * self.fast + (y - shift) % self.fast)
                for z in range(self.slow) for y in range(self.fast)]
        return lax.ppermute(block, "fs", perm)

    def from_rep(self, block, shift):
        return lax.ppermute(block, "rep", [(i, (i - shift) % self.reps) for i in range(self.reps)])

    def from_tp(self, block, shift):
        return lax.ppermute(block, "tp", [(i, (i - shift) % self.tps) for i in range(self.tps)])

    def spread(self, pieces, axis):
        held = jnp.concatenate(pieces, axis)
        held = jnp.concatenate([held] + [self.from_fast(held, j) for j in range(1, self.fast)], axis)
        return jnp.concatenate([held] + [self.from_rep(held, i) for i in range(1, self.reps)], axis)

    def order(self, width):
        return [
            (((self.z + k) % self.slow * self.fast + (self.y + j) % self.fast) * self.reps
             + (self.r + i) % self.reps) * width
            for i in range(self.reps) for j in range(self.fast) for k in range(self.slow)
        ]

    def position(self, block):
        f, part = block // self.reps, block % self.reps
        i = (part - self.r) % self.reps
        j = (f % self.fast - self.y) % self.fast
        k = (f // self.fast - self.z) % self.slow
        return (i * self.fast + j) * self.slow + k


def columns(values, offsets, width):
    return jnp.concatenate(
        [lax.dynamic_slice(values, (0, offset), (values.shape[0], width)) for offset in offsets], axis=1
    )


def inverse_norm(place, values):
    own = jnp.sum(values * values, axis=1)
    total = own
    for s in range(1, place.tps):
        total = total + place.from_tp(own, s)
    return lax.rsqrt(total / (values.shape[1] * place.tps) + epsilon)


def normalize(place, token_rows, gain):
    values = token_rows.astype(jnp.float32)
    return (values * inverse_norm(place, values)[:, None] * gain).astype(low)


def all_features(place, local, width):
    held = jnp.concatenate([local] + [place.from_tp(local, s) for s in range(1, place.tps)], axis=1)
    whole = held.shape[1]
    offsets = [(offset - place.t * local.shape[1]) % whole for offset in place.order(width)]
    return columns(held, offsets, width)


def own_features(place, product, width):
    local = product.shape[1] // place.tps
    count = local // width

    def share(peer):
        return columns(product, [place.position(peer * count + b) * width for b in range(count)], width)

    total = share(place.t)
    for s in range(1, place.tps):
        total = total + place.from_tp(share((place.t - s) % place.tps).astype(low), s).astype(jnp.float32)
    return total


def causal_taps(values, taps):
    tap_count = taps.shape[0]
    grouped = values.reshape(-1, LEN, values.shape[1])
    padded = jnp.pad(grouped, ((0, 0), (tap_count - 1, 0), (0, 0)))
    running = jnp.zeros_like(grouped)
    for offset in range(tap_count):
        running = running + taps[offset] * padded[:, offset : offset + LEN]
    return running.reshape(values.shape)


def dot(left, right):
    return jnp.dot(left, right, preferred_element_type=jnp.float32)


def per_device(
    tokens, mixer_gain, outer_weight, inner_weight, value_weight, outer_scale, inner_scale,
    value_scale, mixer_taps, mixer_project, project_scale, channel_gain, gate_weight, gate_scale,
    up_weight, up_scale, channel_taps, channel_bias, down_weight, down_scale,
):
    sizes = Sizes(
        tuple(lax.axis_size(a) for a in ("rep", "fs", "tp")), tokens, outer_weight, gate_weight, mixer_project
    )
    if sizes.fits(mixer_project):
        return in_one_kernel(
            sizes, tokens, mixer_gain, outer_weight, inner_weight, value_weight, outer_scale, inner_scale,
            value_scale, mixer_taps, mixer_project, project_scale, channel_gain, gate_weight, gate_scale,
            up_weight, up_scale, channel_taps, channel_bias, down_weight, down_scale,
        )
    place = Place()
    rows = outer_weight.shape[0] // place.reps
    width = mixer_project.shape[1] // place.reps
    slow = place.slow
    quarter = gate_weight.shape[1] // slow

    def row_share(weight):
        return lax.dynamic_slice_in_dim(weight, place.r * rows, rows, 0).astype(low)

    def column_share(weight):
        return lax.dynamic_slice_in_dim(weight, place.r * width, width, 1).astype(low)

    def same(piece):
        return [piece] + [place.from_slow(piece, k) for k in range(1, slow)]

    def exchange(take):
        return [take(place.z)] + [
            place.from_slow(take((place.z - k) % slow), k) for k in range(1, slow)
        ]

    mixer_in = place.spread(
        same(jnp.concatenate([row_share(w) for w in (outer_weight, inner_weight, value_weight)], axis=1)), 0
    )
    project = place.spread(same(column_share(mixer_project)), 1)

    def column_part(weight):
        parts = row_share(weight).reshape(rows, slow, quarter).transpose(1, 0, 2)
        return lambda z: lax.dynamic_index_in_dim(parts, z, 0, keepdims=False)

    gate_full = place.spread(exchange(column_part(gate_weight)), 0)
    up_full = place.spread(exchange(column_part(up_weight)), 0)
    down_share = column_share(down_weight)
    down_full = place.spread(
        exchange(lambda z: lax.dynamic_slice_in_dim(down_share, z * quarter, quarter, 0)), 1
    )

    scales = (outer_scale, inner_scale, value_scale, gate_scale, up_scale, project_scale, down_scale)
    packed = lax.all_gather(jnp.concatenate(scales), "fs", axis=0)
    ends, full = 0, []
    for scale in scales:
        full.append(packed[:, ends : ends + scale.shape[0]].reshape(-1))
        ends += scale.shape[0]
    outer_all, inner_all, value_all, gate_all, up_all, project_all, down_all = full
    local = tokens.shape[1]

    def mine(vector, at, size):
        return lax.dynamic_slice_in_dim(vector, at * size, size, vector.ndim - 1)

    normed = all_features(place, normalize(place, tokens, mixer_gain), rows)
    parts = dot(normed, mixer_in)
    each = outer_weight.shape[1]
    outer_part = parts[:, :each] * outer_all
    conv_input = parts[:, each : 2 * each] * inner_all * (parts[:, 2 * each :] * value_all)
    mixed = (outer_part * causal_taps(conv_input, mixer_taps)).astype(low)
    mixer_sum = own_features(place, dot(mixed, project), width) * mine(project_all, place.t, local)
    middle = (tokens.astype(jnp.float32) + mixer_sum).astype(low)

    normed_own = normalize(place, middle, channel_gain)
    normed_two = jnp.concatenate(
        [normed_own] + [place.from_slow(normed_own, k) for k in range(1, slow)], axis=0
    )
    normed_two = all_features(place, normed_two, rows)
    gate_part = dot(normed_two, gate_full) * mine(gate_all, place.z, quarter)
    up_part = dot(normed_two, up_full) * mine(up_all, place.z, quarter)
    hidden = (
        jax.nn.silu(
            causal_taps(gate_part, mine(channel_taps, place.z, quarter))
            + mine(channel_bias, place.z, quarter)
        )
        * up_part
    ).astype(low)
    share = own_features(place, dot(hidden, down_full), width)
    count = tokens.shape[0]
    total = share[:count]
    for k in range(1, slow):
        sent = share[k * count : (k + 1) * count].astype(low)
        total = total + place.from_slow(sent, -k).astype(jnp.float32)
    return (middle.astype(jnp.float32) + total * mine(down_all, place.t, local)).astype(low)


class Sizes:
    def __init__(self, mesh_sizes, tokens, outer_weight, gate_weight, mixer_project):
        self.reps, self.fs, self.tps = mesh_sizes
        self.rows, self.half = tokens.shape
        self.depth, self.cols = outer_weight.shape
        self.block = self.depth // 2
        self.chan = self.cols // 2
        self.quarter = gate_weight.shape[1] // GROUPS
        self.full = self.quarter // LANES
        self.tail = self.quarter % LANES
        self.padded = (self.full + 1) * LANES
        self.wide = 2 * self.quarter
        self.per_half = self.fs // 2
        self.features = self.half * self.tps
        each = self.chan // self.per_half
        self.slots = [0]
        for width in [each] * 3 + [self.quarter // 2] * 2 + [self.depth] * 2:
            self.slots.append(self.slots[-1] + -(-width // LANES) * LANES)
        self.halves = 2 * each == LANES and 2 * (self.slots[4] - self.slots[3]) == self.padded

    def fits(self, mixer_project):
        return (
            (self.reps, self.fs, self.tps) == (2, 2 * GROUPS, 2)
            and self.rows == LEN
            and self.depth % (2 * LANES) == 0
            and self.per_half * self.depth == self.half
            and self.cols == 4 * self.block
            and self.halves
            and self.tail == LANES // 2
            and self.quarter % 32 == 0
            and mixer_project.shape[1] == self.depth
        )


def layer_kernel(
    n, tok_h, mg, cg, mt, channel_taps, channel_bias, s_o, s_i, s_v, s_g, s_u, s_p, s_d,
    ow, iw, vw, pw, gw, uw, dn, out,
    tok, st_m, st_p, st_g, st_u, st_d, mw, ms, gu, dw, sg, sd, pk, sc, msc, gsus, ct, sq, sqr,
    xg, mps, mpr, ys, yr, mid, ng, hid, acc, ps, pr, zs, zb, za, lsem, ss, rs,
):
    f32 = jnp.float32
    zn = GROUPS
    r, f, t = lax.axis_index("rep"), lax.axis_index("fs"), lax.axis_index("tp")
    z, y = f // 2, f % 2
    py, px, pt = (r, f + 1 - 2 * y, t), (1 - r, f, t), (r, f, 1 - t)
    fy = 2 * z + 1 - y
    up, down = (r, (f + 2) % n.fs, t), (r, (f + n.fs - 2) % n.fs, t)
    can_up, can_down = z < zn - 1, z > 0
    inner = (z > 0) & (z < zn - 1)
    ends = (z == 0) | (z == zn - 1)
    D, B, CH, Q = n.depth, n.block, n.chan, n.quarter

    used = [0]
    pending = []

    def ids(count=1):
        used[0] += count
        return used[0] - count

    def when(cond, fn):
        if cond is None:
            fn()
        else:
            pl.when(cond)(fn)

    def send(src, dst, sid, rid, dev, cond=None):
        c = pltpu.make_async_remote_copy(
            src_ref=src, dst_ref=dst, send_sem=ss.at[sid], recv_sem=rs.at[rid],
            device_id=dev, device_id_type=MESH,
        )
        when(cond, c.start)
        pending.append((c, cond))

    def arrive(dst, rid, cond=None):
        c = pltpu.make_async_remote_copy(
            src_ref=dst, dst_ref=dst, send_sem=ss.at[0], recv_sem=rs.at[rid],
            device_id=pt, device_id_type=MESH,
        )
        when(cond, c.wait_recv)

    def place(fb, rh):
        return pl.multiple_of((fb // n.per_half) * n.half + rh * (n.half // 2) + (fb % n.per_half) * B, B)

    def dot(a, b):
        return jnp.dot(a, b, preferred_element_type=f32)

    def conv(v, w0, w1, w2):
        at = lax.broadcasted_iota(jnp.int32, v.shape, 0)
        one = jnp.where(at >= 1, pltpu.roll(v, 1, axis=0), 0.0)
        two = jnp.where(at >= 2, pltpu.roll(v, 2, axis=0), 0.0)
        return w0 * two + w1 * one + w2 * v

    loads = []

    def load(src, dst):
        c = pltpu.make_async_copy(src, dst, lsem.at[len(loads)])
        c.start()
        loads.append(c)
        return c

    load_tok = load(tok_h, tok)
    load_m = []
    for m, w in enumerate((ow, iw, vw)):
        for h in range(2):
            load_m.append(load(w.at[:, h * CH:(h + 1) * CH], st_m.at[m, h]))
    load_m.append(load(pw, st_p))
    load_f = [load(gw, st_g), load(uw, st_u), load(dn, st_d)]

    barrier = pltpu.get_barrier_semaphore()
    for k in range(1, n.fs):
        pl.semaphore_signal(barrier, inc=1, device_id=(r, (f + k) % n.fs, t), device_id_type=MESH)
    pl.semaphore_signal(barrier, inc=1, device_id=px, device_id_type=MESH)
    pl.semaphore_signal(barrier, inc=1, device_id=pt, device_id_type=MESH)

    for c in load_m:
        c.wait()
    for rh in range(2):
        here = slice(rh * B, (rh + 1) * B)
        for m in range(3):
            ms[here, m * CH:(m + 1) * CH] = st_m[m, 1 - y, here, :].astype(low)
            mw[pl.ds(place(f, rh), B), m * CH:(m + 1) * CH] = st_m[m, y, here, :].astype(low)
        for h, ref, rows in ((1 - y, ms, here), (y, mw, pl.ds(place(f, rh), B))):
            ref[rows, 3 * CH:] = st_p[pl.ds(pl.multiple_of(h * CH + rh * B, B), B), :].astype(low)

    pk[...] = jnp.zeros_like(pk)
    for at, ref in zip(n.slots, (s_o, s_i, s_v, s_g, s_u, s_p, s_d)):
        pk[:, at:at + ref.shape[0]] = ref[...][None, :]
    for q in range(zn):
        @pl.when(z == q)
        def _():
            base = q * Q // LANES * LANES
            for ref, rows in ((channel_taps, slice(0, 3)), (channel_bias, slice(3, 4))):
                taps = ref[:, base:base + n.padded] if len(ref.shape) == 2 else ref[base:base + n.padded][None, :]
                ct[rows, :] = pltpu.roll(taps, n.padded - LANES // 2, axis=1) if q * Q % LANES else taps

    load_tok.wait()

    def square_sum(values):
        return jnp.sum(values * values, axis=1, keepdims=True)

    sq_id = ids(2)

    def share_squares(which, total):
        sq[which] = jnp.broadcast_to(total, (n.rows, LANES))
        send(sq.at[which], sqr.at[which], sq_id + which, sq_id + which, pt)

    own_squares = square_sum(tok[...].astype(f32))
    pl.semaphore_wait(barrier, n.fs + 1)
    share_squares(0, own_squares)

    m1 = ids(2)

    def block_at(fb, rh):
        return mw.at[pl.ds(place(fb, rh), B)]

    def send_m1(rh):
        send(ms.at[pl.ds(pl.multiple_of(rh * B, B), B)], block_at(f, rh), m1 + rh, m1 + rh, py)

    def arrive_m1(rh):
        arrive(block_at(fy, rh), m1 + rh)

    send_m1(r)

    class Line:
        def __init__(self, block):
            self.block = block
            self.up, self.down, self.below, self.above = ids(zn), ids(zn), ids(zn), ids(zn)

        def forward(self, at, k, upward, cond):
            b = self.block(at)
            send(b, b, (self.up if upward else self.down) + k, (self.below if upward else self.above) + k + 1,
                 up if upward else down, cond)

        def start(self):
            self.forward(z, 0, True, can_up)
            self.forward(z, 0, False, can_down)

        def step(self, k, then):
            a, b = (z + zn - k) % zn, (z + k) % zn
            for at, base, upward, cond, more in (
                (a, self.below, True, z >= k, can_up), (b, self.above, False, z < zn - k, can_down),
            ):
                arrive(self.block(at), base + k, cond)
                if k < zn - 1:
                    self.forward(at, k, upward, cond & more)
                then(at, k, upward, cond)

    own_line = Line(lambda at: block_at(2 * at + y, r))
    other_line = Line(lambda at: block_at(2 * at + 1 - y, r))
    own_line.start()

    def inverse_norm_of(which, own):
        arrive(sqr.at[which], sq_id + which)
        return lax.rsqrt((own + sqr[which][:, :1]) / n.features + epsilon)

    def normalize(values, rows, inverse, gain, dst):
        for fl in range(n.per_half):
            for rh in range(2):
                here = slice((2 * fl + rh) * B, (2 * fl + rh + 1) * B)
                there = slice((rh * n.per_half + fl) * B, (rh * n.per_half + fl + 1) * B)
                dst[rows, there] = (values[rows, here].astype(f32) * inverse[rows] * gain[:, here]).astype(low)

    whole = slice(0, n.rows)
    parts = [slice(c * n.rows // 2, (c + 1) * n.rows // 2) for c in range(2)]

    normalize(tok, whole, inverse_norm_of(0, own_squares), mg, xg.at[y, t])
    x_y, x_t = ids(), ids(2)
    send(xg.at[y, t], xg.at[y, t], x_y, x_y, py)
    send(xg.at[y, t], xg.at[y, t], x_t, x_t, pt)
    send_m1(1 - r)

    scale_s, scale_r = ids(n.fs), ids(n.fs)
    sc[f] = pk[...]
    for k in range(1, n.fs):
        send(pk, sc.at[f], scale_s + k, scale_r + f, (r, (f + k) % n.fs, t))

    mx = ids(4 * zn)

    def over_x(which, blk):
        def then(at, k, upward, cond):
            s = mx + 4 * k + 2 * which + (1 if upward else 0)
            send(blk(at), blk(at), s, s, px, cond)
        return then

    for c in load_f:
        c.wait()

    def tiles(rows, q):
        base = q * Q // LANES * LANES
        g = st_g[rows, base:base + n.padded]
        u = st_u[rows, base:base + n.padded]
        if q * Q % LANES:
            g = pltpu.roll(g, n.padded - LANES // 2, axis=1)
            u = pltpu.roll(u, n.padded - LANES // 2, axis=1)
        parts = []
        for j in range(n.full):
            parts += [g[:, j * LANES:(j + 1) * LANES], u[:, j * LANES:(j + 1) * LANES]]
        lane = lax.broadcasted_iota(jnp.int32, (B, LANES), 1)
        parts.append(jnp.where(lane < LANES // 2, g[:, n.full * LANES:], pltpu.roll(u[:, n.full * LANES:], LANES // 2, axis=1)))
        return parts

    for q in range(zn):
        @pl.when(z == q)
        def _():
            for rh in range(2):
                for j, piece in enumerate(tiles(pl.ds(rh * B, B), q)):
                    gu[pl.ds(place(f, rh), B), j * LANES:(j + 1) * LANES] = piece.astype(low)

        @pl.when(z != q)
        def _():
            for j, piece in enumerate(tiles(pl.ds(pl.multiple_of(r * B, B), B), q)):
                sg[q, :, j * LANES:(j + 1) * LANES] = piece.astype(low)

        sd[q] = st_d[pl.ds(pl.multiple_of(q * Q + r * (Q // 2), 16), Q // 2), :].astype(low)
    dw[f] = st_d[pl.ds(pl.multiple_of(z * Q, 16), Q), :].astype(low)

    def gu_at(fb, rh):
        return gu.at[pl.ds(place(fb, rh), B)]

    def dw_at(fb, rh):
        return dw.at[fb, pl.ds(pl.multiple_of(rh * (Q // 2), 16), Q // 2)]

    fy_own = ids(4)
    for rh in range(2):
        send(gu_at(f, rh), gu_at(f, rh), fy_own + rh, fy_own + rh, py)
    send(dw_at(f, r), dw_at(f, r), fy_own + 2, fy_own + 2, py)

    f1, f2y, f2x, f2d = ids(2 * zn), ids(2 * zn), ids(2 * zn), ids(2 * zn)

    def across(k):
        if k == 1:
            return z + 1 - 2 * (z % 2)
        if k == 2:
            return z + 2 - 4 * (z // 2)
        return zn - 1 - z

    def stage_one(k, cond):
        q = across(k)
        dev = (r, 2 * q + y, t)
        send(sg.at[q], gu_at(f, r), f1 + 2 * k, f1 + 2 * k, dev, cond)
        send(sd.at[q], dw_at(f, r), f1 + 2 * k + 1, f1 + 2 * k + 1, dev, cond)

    def held(k):
        fb = 2 * across(k) + y
        return enumerate((gu_at(fb, r), dw_at(fb, r)))

    def pieces_over_x(k, cond):
        for i, ref in held(k):
            arrive(ref, f1 + 2 * k + i, cond)
            send(ref, ref, f2x + 2 * k + i, f2x + 2 * k + i, px, cond)

    def pieces_over_y(k):
        for i, ref in held(k):
            send(ref, ref, f2y + 2 * k + i, f2y + 2 * k + i, py)

    def over_y(k, i):
        return k == zn - 1

    def refs_of(k, own_y, rh):
        fb = 2 * across(k) + (y if own_y else 1 - y)
        return gu_at(fb, rh), dw_at(fb, rh)

    def pieces_on(k):
        for i in range(2):
            if over_y(k, i):
                ref, base, dev = refs_of(k, True, 1 - r)[i], f2x, py
            else:
                ref, base, dev = refs_of(k, False, r)[i], f2y, px
            arrive(ref, base + 2 * k + i)
            send(ref, ref, f2d + 2 * k + i, f2d + 2 * k + i, dev)

    def pieces_end(k, i):
        if over_y(k, i):
            arrive(refs_of(k, False, r)[i], f2y + 2 * k + i)
        else:
            arrive(refs_of(k, True, 1 - r)[i], f2x + 2 * k + i)
        arrive(refs_of(k, False, 1 - r)[i], f2d + 2 * k + i)

    arrive_m1(r)
    other_line.start()
    stage_one(1, ends)
    own_x, other_x = over_x(0, own_line.block), over_x(1, other_line.block)
    own_line.step(1, own_x)
    other_line.step(1, other_x)
    own_line.step(2, own_x)
    arrive(xg.at[1 - y, t], x_y)
    send(xg.at[1 - y, t], xg.at[1 - y, t], x_t + 1, x_t + 1, pt)
    other_line.step(2, other_x)
    stage_one(2, ends)
    stage_one(3, inner)
    own_line.step(3, own_x)
    other_line.step(3, other_x)

    for k in range(1, n.fs):
        fk = (f + k) % n.fs
        arrive(sc.at[fk], scale_r + fk)
    for m, at in enumerate(n.slots[:3]):
        slot = slice(at, at + LANES)
        for j in range(CH // LANES):
            fb = n.per_half * y + 2 * j
            msc[m:m + 1, j * LANES:(j + 1) * LANES] = sc[fb][:, slot] + pltpu.roll(sc[fb + 1][:, slot], LANES // 2, axis=1)
    for i, at in enumerate(n.slots[3:5]):
        first, second = (
            jnp.concatenate([sc[2 * z + h][:, at:at + n.padded // 2], jnp.zeros((1, n.padded // 2), f32)], axis=1)
            for h in range(2)
        )
        gsus[i:i + 1, :] = first + pltpu.roll(second, Q // 2, axis=1)
    arrive_m1(1 - r)
    for i in range(2):
        arrive(xg.at[y if i == 0 else 1 - y, 1 - t], x_t + i)
    near = z // 2

    def arrive_mixer(k, own_half, streams=(0, 1)):
        for side, at, cond in ((1, (z + zn - k) % zn, z >= k), (0, (z + k) % zn, z < zn - k)):
            for which in streams:
                fb = 2 * at + (1 - y if which else y)
                same = at // 2 == near
                arrive(block_at(fb, 1 - r), mx + 4 * k + 2 * which + side, cond & (same if own_half else ~same))

    arrive_mixer(1, True)
    near_rows = pl.ds(pl.multiple_of(near * n.half, n.half), n.half)
    far_rows = pl.ds(pl.multiple_of((1 - near) * n.half, n.half), n.half)
    for i, sy in enumerate((1 - y, y)):
        for m in range(3):
            here = slice(m * CH, (m + 1) * CH)
            acc[2 + i, :, here] = dot(xg[sy, near], mw[near_rows, here])
    arrive_mixer(1, False)
    stage_one(1, inner)
    arrive_mixer(2, False)
    arrive_mixer(3, False)

    y_lanes = pl.ds(pl.multiple_of(y * CH, CH), CH)
    m_taps = [mt[k:k + 1, y_lanes] for k in range(3)]
    mt_id, my_id = ids(3), ids(2)
    pad = 16

    def wide(fl):
        return slice(fl * D, (fl + 1) * D)

    def with_past(rows):
        first = max(rows.start - pad, 0)
        return slice(first, rows.stop), rows.start - first

    def mix(i, rows, at):
        sy = (1 - y, y)[i]
        long, drop = with_past(rows)

        def part(m):
            here = slice(m * CH, (m + 1) * CH)
            return (acc[2 + i, long, here] + dot(xg[sy, 1 - near, long], mw[far_rows, here])) * msc[m:m + 1, :]

        cv = conv(part(1) * part(2), *m_taps)
        mixed = (part(0) * cv).astype(low)[drop:]

        def project(fb):
            return dot(mixed, jnp.concatenate([mw[pl.ds(place(fb, rh), B), 3 * CH:] for rh in range(2)], axis=0))

        for fl in range(n.per_half):
            mps[i, rows, wide(fl)] = project(n.per_half * (1 - t) + fl).astype(low)
        send(mps.at[i, rows], mpr.at[i, rows], mt_id + at, mt_id + at, pt)
        for fl in range(n.per_half):
            acc[i, rows, wide(fl)] = project(n.per_half * t + fl)

    for c, rows in enumerate(parts):
        if c == 1:
            pieces_over_x(1, ends)
        mix(0, rows, c)
        arrive(mpr.at[0, rows], mt_id + c)
        ys[rows] = (acc[0, rows] + mpr[0, rows].astype(f32)).astype(low)
        send(ys.at[rows], yr.at[rows], my_id + c, my_id + c, py)
    stage_one(2, inner)
    arrive(dw_at(fy, r), fy_own + 2)
    send(dw_at(fy, r), dw_at(fy, r), fy_own + 3, fy_own + 3, px)
    pieces_over_x(1, inner)
    mix(1, whole, 2)
    arrive(mpr.at[1], mt_id + 2)

    pieces_over_x(3, inner)
    pieces_over_x(2, inner)

    pieces_over_y(1)
    arrive(yr.at[parts[0]], my_id)
    stage_one(3, ends)
    arrive(yr.at[parts[1]], my_id + 1)
    pieces_over_x(2, ends)
    total_sq = None
    for fl in range(n.per_half):
        w = wide(fl)
        added = (acc[1, :, w] + mpr[1, :, w].astype(f32) + yr[:, w].astype(f32)) * sc[n.per_half * t + fl][:, n.slots[5]:n.slots[5] + D]
        middle = (tok[:, w].astype(f32) + added).astype(low)
        mid[:, w] = middle
        part_sq = square_sum(middle.astype(f32))
        total_sq = part_sq if total_sq is None else total_sq + part_sq
    share_squares(1, total_sq)
    inverse = inverse_norm_of(1, total_sq)

    n_t = ids(4 * zn)
    token_lines = []
    for c, rows in enumerate(parts):
        normalize(mid, rows, inverse, cg, ng.at[z, t])
        line = Line(lambda at, rows=rows: ng.at[at, t, rows])
        line.start()
        token_lines.append(line)
        send(line.block(z), line.block(z), n_t + c, n_t + c, pt)

    def token_step(k):
        for c, line in enumerate(token_lines):
            def to_core(at, k, upward, cond):
                s = n_t + 4 * k + (2 if upward else 0) + c
                send(line.block(at), line.block(at), s, s, pt, cond)

            line.step(k, to_core)

    pieces_over_y(2)
    pieces_over_x(3, ends)
    pieces_over_y(3)
    pieces_on(1)
    token_step(1)
    pieces_on(2)
    pieces_on(3)
    token_step(2)
    def core_step(k):
        for c, rows in enumerate(parts):
            for side, at, cond in ((2, (z + zn - k) % zn, z >= k), (0, (z + k) % zn, z < zn - k)):
                arrive(ng.at[at, 1 - t, rows], n_t + 4 * k + side + c, cond)

    for c, rows in enumerate(parts):
        arrive(ng.at[z, 1 - t, rows], n_t + c)
    core_step(1)
    core_step(2)
    for rh in range(2):
        arrive(gu_at(fy, rh), fy_own + rh)
    for k in range(1, zn):
        pieces_end(k, 0)

    p_t, z_s, z_b, z_a = ids(6), ids(2 * zn), ids(2 * zn), ids(2 * zn)
    side = z // 2
    order = (2 - side, 3 * (1 - side), z + 1 - 2 * (z % 2), z)

    def to_line(i, c, cond_up, cond_down):
        s, here = order[i], parts[c]
        for dst, base, dev, cond in ((zb, z_b, up, cond_up), (za, z_a, down, cond_down)):
            send(zs.at[s, here], dst.at[s, here], z_s + 2 * i + c, base + 2 * s + c, dev, cond)

    def chain(i, c):
        s, here = order[i], parts[c]
        for ref, base, cond in ((zb, z_b, inner & (s > z)), (za, z_a, inner & (s < z))):
            arrive(ref.at[s, here], base + 2 * s + c, cond)

            @pl.when(cond)
            def _():
                zs[s, here] = (acc[i, here] + ref[s, here].astype(f32)).astype(low)

        to_line(i, c, inner & (s > z), inner & (s < z))

    def gated(a, here):
        c = conv(a * gsus[0:1, here], ct[0:1, here], ct[1:2, here], ct[2:3, here]) + ct[3:4, here]
        return c / (1.0 + jnp.exp(-c))

    def hidden(s, rows):
        long, drop = with_past(rows)

        def product(at, width):
            here = slice(at, at + width)
            return dot(ng[s, 0, long], gu[:n.half, here]) + dot(ng[s, 1, long], gu[n.half:, here])

        for j in range(n.full):
            a = product(j * 2 * LANES, 2 * LANES)
            here = slice(j * LANES, (j + 1) * LANES)
            hid[rows, here] = (gated(a[:, :LANES], here) * (a[:, LANES:] * gsus[1:2, here])).astype(low)[drop:]
        a = product(n.full * 2 * LANES, LANES)
        here = slice(n.full * LANES, n.padded)
        last = gated(a, here) * (pltpu.roll(a, LANES // 2, axis=1) * gsus[1:2, here])
        hid[rows, n.full * LANES:] = last.astype(low)[drop:, :n.tail]

    def back(i, rows, at):
        hid_v = hid[rows]
        for fl in range(n.per_half):
            ps[i, rows, wide(fl)] = dot(hid_v, dw[n.per_half * (1 - t) + fl]).astype(low)
        send(ps.at[i, rows], pr.at[i, rows], p_t + at, p_t + at, pt)
        for fl in range(n.per_half):
            acc[i, rows, wide(fl)] = dot(hid_v, dw[n.per_half * t + fl])
        arrive(pr.at[i, rows], p_t + at)
        acc[i, rows] = acc[i, rows] + pr[i, rows].astype(f32)
        if i < zn - 1:
            @pl.when(ends)
            def _():
                zs[order[i], rows] = acc[i, rows].astype(low)

    def outward(i, c):
        to_line(i, c, z == 0, z == zn - 1)

    hidden(order[0], parts[0])
    arrive(dw_at(fy, 1 - r), fy_own + 3)
    for k in range(1, zn):
        pieces_end(k, 1)
    back(0, parts[0], 0)
    outward(0, 0)
    hidden(order[0], parts[1])
    back(0, parts[1], 1)
    token_step(3)
    core_step(3)
    for c in range(2):
        hidden(order[1], parts[c])
        back(1, parts[c], 2 + c)
        outward(1, c)
    outward(0, 1)
    hidden(order[2], whole)
    back(2, whole, 4)
    outward(2, 0)
    outward(2, 1)
    chain(0, 0)
    chain(1, 0)
    hidden(order[3], whole)
    back(3, whole, 5)
    for i, c in ((1, 1), (2, 0), (0, 1), (2, 1)):
        chain(i, c)

    for c, here in enumerate(parts):
        for ref, base, cond in ((zb, z_b, can_down), (za, z_a, can_up)):
            arrive(ref.at[z, here], base + 2 * z + c, cond)

            @pl.when(cond)
            def _():
                acc[zn - 1, here] = acc[zn - 1, here] + ref[z, here].astype(f32)

    for fl in range(n.per_half):
        w = wide(fl)
        scaled = acc[zn - 1, :, w] * sc[n.per_half * t + fl][:, n.slots[6]:n.slots[6] + D]
        out[:, w] = (mid[:, w].astype(f32) + scaled).astype(low)

    for c, cond in pending:
        when(cond, c.wait_send)
    assert used[0] <= SEMAPHORES, used[0]


def in_one_kernel(
    n, tokens, mixer_gain, outer_weight, inner_weight, value_weight, outer_scale, inner_scale,
    value_scale, mixer_taps, mixer_project, project_scale, channel_gain, gate_weight, gate_scale,
    up_weight, up_scale, channel_taps, channel_bias, down_weight, down_scale,
):
    f32, zn = jnp.float32, GROUPS
    scales = (outer_scale, inner_scale, value_scale, gate_scale, up_scale, project_scale, down_scale)
    vm, anywhere = pl.BlockSpec(memory_space=pltpu.VMEM), pl.BlockSpec(memory_space=pl.ANY)
    rows, half, features = n.rows, n.half, n.features

    def V(shape, dtype=low):
        return pltpu.VMEM(shape, dtype)

    scratch = [
        V((rows, half)),
        V((3, 2, n.depth, n.chan), f32), V((n.cols, n.depth), f32),
        V((n.depth, zn * n.quarter), f32), V((n.depth, zn * n.quarter), f32), V((zn * n.quarter, n.depth), f32),
        V((features, 3 * n.chan + n.depth)), V((n.depth, 3 * n.chan + n.depth)),
        V((features, n.wide)), V((n.fs, n.quarter, n.depth)),
        V((zn, n.block, n.wide)), V((zn, n.quarter // 2, n.depth)),
        V((1, n.slots[-1]), f32), V((n.fs, 1, n.slots[-1]), f32), V((3, n.chan), f32), V((2, n.padded), f32), V((4, n.padded), f32),
        V((2, rows, LANES), f32), V((2, rows, LANES), f32),
        V((2, 2, rows, half)), V((2, rows, half)), V((2, rows, half)), V((rows, half)), V((rows, half)),
        V((rows, half)), V((zn, 2, rows, half)), V((rows, n.quarter)), V((zn, rows, half), f32),
        V((zn, rows, half)), V((zn, rows, half)), V((zn, rows, half)), V((zn, rows, half)), V((zn, rows, half)),
        pltpu.SemaphoreType.DMA((16,)), pltpu.SemaphoreType.DMA((SEMAPHORES,)), pltpu.SemaphoreType.DMA((SEMAPHORES,)),
    ]
    return pl.pallas_call(
        functools.partial(layer_kernel, n),
        out_shape=jax.ShapeDtypeStruct(tokens.shape, tokens.dtype),
        in_specs=[anywhere] + [vm] * 12 + [anywhere] * 7,
        out_specs=vm,
        scratch_shapes=scratch,
        compiler_params=pltpu.CompilerParams(
            collective_id=0, has_side_effects=True, vmem_limit_bytes=VMEM_BYTES
        ),
    )(
        tokens, mixer_gain[None, :], channel_gain[None, :], mixer_taps, channel_taps, channel_bias, *scales,
        outer_weight, inner_weight, value_weight, mixer_project, gate_weight, up_weight, down_weight,
    )


def solution(mesh):
    placed = (
        P(("rep", "fs"), "tp"),
        P("tp"),
        P("fs", "tp"),
        P("fs", "tp"),
        P("fs", "tp"),
        P(("tp", "fs")),
        P(("tp", "fs")),
        P(("tp", "fs")),
        P(None, "tp"),
        P("tp", "fs"),
        P("fs"),
        P("tp"),
        P("fs", "tp"),
        P(("tp", "fs")),
        P("fs", "tp"),
        P(("tp", "fs")),
        P(None, "tp"),
        P("tp"),
        P("tp", "fs"),
        P("fs"),
    )
    return jax.shard_map(
        per_device, mesh=mesh, in_specs=placed, out_specs=P(("rep", "fs"), "tp"), check_vma=False
    )
```

```python
import functools

import jax
import jax.numpy as jnp
from jax import lax
from jax.experimental import pallas as pl
from jax.experimental.pallas import tpu as pltpu
from jax.sharding import PartitionSpec as P

LEN = 320
GROUPS = 4
LANES = 128
SEMAPHORES = 256
VMEM_BYTES = 65000 * 1024
MESH = pl.DeviceIdType.MESH

epsilon = 1e-06
low = jnp.bfloat16


class Place:
    def __init__(self):
        self.fs = lax.axis_size("fs")
        self.reps = lax.axis_size("rep")
        self.tps = lax.axis_size("tp")
        self.slow = GROUPS if self.fs % GROUPS == 0 else 1
        self.fast = self.fs // self.slow
        at = lax.axis_index("fs")
        self.z, self.y = at // self.fast, at % self.fast
        self.r, self.t = lax.axis_index("rep"), lax.axis_index("tp")

    def from_slow(self, block, shift):
        perm = [(z * self.fast + y, (z - shift) % self.slow * self.fast + y)
                for z in range(self.slow) for y in range(self.fast)]
        return lax.ppermute(block, "fs", perm)

    def from_fast(self, block, shift):
        perm = [(z * self.fast + y, z * self.fast + (y - shift) % self.fast)
                for z in range(self.slow) for y in range(self.fast)]
        return lax.ppermute(block, "fs", perm)

    def from_rep(self, block, shift):
        return lax.ppermute(block, "rep", [(i, (i - shift) % self.reps) for i in range(self.reps)])

    def from_tp(self, block, shift):
        return lax.ppermute(block, "tp", [(i, (i - shift) % self.tps) for i in range(self.tps)])

    def spread(self, pieces, axis):
        held = jnp.concatenate(pieces, axis)
        held = jnp.concatenate([held] + [self.from_fast(held, j) for j in range(1, self.fast)], axis)
        return jnp.concatenate([held] + [self.from_rep(held, i) for i in range(1, self.reps)], axis)

    def order(self, width):
        return [
            (((self.z + k) % self.slow * self.fast + (self.y + j) % self.fast) * self.reps
             + (self.r + i) % self.reps) * width
            for i in range(self.reps) for j in range(self.fast) for k in range(self.slow)
        ]

    def position(self, block):
        f, part = block // self.reps, block % self.reps
        i = (part - self.r) % self.reps
        j = (f % self.fast - self.y) % self.fast
        k = (f // self.fast - self.z) % self.slow
        return (i * self.fast + j) * self.slow + k


def columns(values, offsets, width):
    return jnp.concatenate(
        [lax.dynamic_slice(values, (0, offset), (values.shape[0], width)) for offset in offsets], axis=1
    )


def inverse_norm(place, values):
    own = jnp.sum(values * values, axis=1)
    total = own
    for s in range(1, place.tps):
        total = total + place.from_tp(own, s)
    return lax.rsqrt(total / (values.shape[1] * place.tps) + epsilon)


def normalize(place, token_rows, gain):
    values = token_rows.astype(jnp.float32)
    return (values * inverse_norm(place, values)[:, None] * gain).astype(low)


def all_features(place, local, width):
    held = jnp.concatenate([local] + [place.from_tp(local, s) for s in range(1, place.tps)], axis=1)
    whole = held.shape[1]
    offsets = [(offset - place.t * local.shape[1]) % whole for offset in place.order(width)]
    return columns(held, offsets, width)


def own_features(place, product, width):
    local = product.shape[1] // place.tps
    count = local // width

    def share(peer):
        return columns(product, [place.position(peer * count + b) * width for b in range(count)], width)

    total = share(place.t)
    for s in range(1, place.tps):
        total = total + place.from_tp(share((place.t - s) % place.tps).astype(low), s).astype(jnp.float32)
    return total


def causal_taps(values, taps):
    tap_count = taps.shape[0]
    grouped = values.reshape(-1, LEN, values.shape[1])
    padded = jnp.pad(grouped, ((0, 0), (tap_count - 1, 0), (0, 0)))
    running = jnp.zeros_like(grouped)
    for offset in range(tap_count):
        running = running + taps[offset] * padded[:, offset : offset + LEN]
    return running.reshape(values.shape)


def dot(left, right):
    return jnp.dot(left, right, preferred_element_type=jnp.float32)


def per_device(
    tokens, mixer_gain, outer_weight, inner_weight, value_weight, outer_scale, inner_scale,
    value_scale, mixer_taps, mixer_project, project_scale, channel_gain, gate_weight, gate_scale,
    up_weight, up_scale, channel_taps, channel_bias, down_weight, down_scale,
):
    sizes = Sizes(
        tuple(lax.axis_size(a) for a in ("rep", "fs", "tp")), tokens, outer_weight, gate_weight, mixer_project
    )
    if sizes.fits(mixer_project):
        return in_one_kernel(
            sizes, tokens, mixer_gain, outer_weight, inner_weight, value_weight, outer_scale, inner_scale,
            value_scale, mixer_taps, mixer_project, project_scale, channel_gain, gate_weight, gate_scale,
            up_weight, up_scale, channel_taps, channel_bias, down_weight, down_scale,
        )
    place = Place()
    rows = outer_weight.shape[0] // place.reps
    width = mixer_project.shape[1] // place.reps
    slow = place.slow
    quarter = gate_weight.shape[1] // slow

    def row_share(weight):
        return lax.dynamic_slice_in_dim(weight, place.r * rows, rows, 0).astype(low)

    def column_share(weight):
        return lax.dynamic_slice_in_dim(weight, place.r * width, width, 1).astype(low)

    def same(piece):
        return [piece] + [place.from_slow(piece, k) for k in range(1, slow)]

    def exchange(take):
        return [take(place.z)] + [
            place.from_slow(take((place.z - k) % slow), k) for k in range(1, slow)
        ]

    mixer_in = place.spread(
        same(jnp.concatenate([row_share(w) for w in (outer_weight, inner_weight, value_weight)], axis=1)), 0
    )
    project = place.spread(same(column_share(mixer_project)), 1)

    def column_part(weight):
        parts = row_share(weight).reshape(rows, slow, quarter).transpose(1, 0, 2)
        return lambda z: lax.dynamic_index_in_dim(parts, z, 0, keepdims=False)

    gate_full = place.spread(exchange(column_part(gate_weight)), 0)
    up_full = place.spread(exchange(column_part(up_weight)), 0)
    down_share = column_share(down_weight)
    down_full = place.spread(
        exchange(lambda z: lax.dynamic_slice_in_dim(down_share, z * quarter, quarter, 0)), 1
    )

    scales = (outer_scale, inner_scale, value_scale, gate_scale, up_scale, project_scale, down_scale)
    packed = lax.all_gather(jnp.concatenate(scales), "fs", axis=0)
    ends, full = 0, []
    for scale in scales:
        full.append(packed[:, ends : ends + scale.shape[0]].reshape(-1))
        ends += scale.shape[0]
    outer_all, inner_all, value_all, gate_all, up_all, project_all, down_all = full
    local = tokens.shape[1]

    def mine(vector, at, size):
        return lax.dynamic_slice_in_dim(vector, at * size, size, vector.ndim - 1)

    normed = all_features(place, normalize(place, tokens, mixer_gain), rows)
    parts = dot(normed, mixer_in)
    each = outer_weight.shape[1]
    outer_part = parts[:, :each] * outer_all
    conv_input = parts[:, each : 2 * each] * inner_all * (parts[:, 2 * each :] * value_all)
    mixed = (outer_part * causal_taps(conv_input, mixer_taps)).astype(low)
    mixer_sum = own_features(place, dot(mixed, project), width) * mine(project_all, place.t, local)
    middle = (tokens.astype(jnp.float32) + mixer_sum).astype(low)

    normed_own = normalize(place, middle, channel_gain)
    normed_two = jnp.concatenate(
        [normed_own] + [place.from_slow(normed_own, k) for k in range(1, slow)], axis=0
    )
    normed_two = all_features(place, normed_two, rows)
    gate_part = dot(normed_two, gate_full) * mine(gate_all, place.z, quarter)
    up_part = dot(normed_two, up_full) * mine(up_all, place.z, quarter)
    hidden = (
        jax.nn.silu(
            causal_taps(gate_part, mine(channel_taps, place.z, quarter))
            + mine(channel_bias, place.z, quarter)
        )
        * up_part
    ).astype(low)
    share = own_features(place, dot(hidden, down_full), width)
    count = tokens.shape[0]
    total = share[:count]
    for k in range(1, slow):
        sent = share[k * count : (k + 1) * count].astype(low)
        total = total + place.from_slow(sent, -k).astype(jnp.float32)
    return (middle.astype(jnp.float32) + total * mine(down_all, place.t, local)).astype(low)


class Sizes:
    def __init__(self, mesh_sizes, tokens, outer_weight, gate_weight, mixer_project):
        self.reps, self.fs, self.tps = mesh_sizes
        self.rows, self.half = tokens.shape
        self.depth, self.cols = outer_weight.shape
        self.block = self.depth // 2
        self.chan = self.cols // 2
        self.quarter = gate_weight.shape[1] // GROUPS
        self.full = self.quarter // LANES
        self.tail = self.quarter % LANES
        self.padded = (self.full + 1) * LANES
        self.wide = 2 * self.quarter
        self.per_half = self.fs // 2
        self.features = self.half * self.tps
        each = self.chan // self.per_half
        self.slots = [0]
        for width in [each] * 3 + [self.quarter // 2] * 2 + [self.depth] * 2:
            self.slots.append(self.slots[-1] + -(-width // LANES) * LANES)
        self.halves = 2 * each == LANES and 2 * (self.slots[4] - self.slots[3]) == self.padded

    def fits(self, mixer_project):
        return (
            (self.reps, self.fs, self.tps) == (2, 2 * GROUPS, 2)
            and self.rows == LEN
            and self.depth % (2 * LANES) == 0
            and self.per_half * self.depth == self.half
            and self.cols == 4 * self.block
            and self.halves
            and self.tail == LANES // 2
            and self.quarter % 32 == 0
            and mixer_project.shape[1] == self.depth
        )


def layer_kernel(
    n, tok_h, mg, cg, mt, channel_taps, channel_bias, s_o, s_i, s_v, s_g, s_u, s_p, s_d,
    ow, iw, vw, pw, gw, uw, dn, out,
    tok, st_m, st_p, st_g, st_u, st_d, mw, ms, gu, dw, sg, sd, pk, sc, msc, gsus, ct, sq, sqr,
    xg, mps, mpr, ys, yr, mid, ng, hid, acc, ps, pr, zs, zb, za, lsem, ss, rs,
):
    f32 = jnp.float32
    zn = GROUPS
    r, f, t = lax.axis_index("rep"), lax.axis_index("fs"), lax.axis_index("tp")
    z, y = f // 2, f % 2
    py, px, pt = (r, f + 1 - 2 * y, t), (1 - r, f, t), (r, f, 1 - t)
    fy = 2 * z + 1 - y
    up, down = (r, (f + 2) % n.fs, t), (r, (f + n.fs - 2) % n.fs, t)
    can_up, can_down = z < zn - 1, z > 0
    inner = (z > 0) & (z < zn - 1)
    ends = (z == 0) | (z == zn - 1)
    D, B, CH, Q = n.depth, n.block, n.chan, n.quarter

    used = [0]
    pending = []

    def ids(count=1):
        used[0] += count
        return used[0] - count

    def when(cond, fn):
        if cond is None:
            fn()
        else:
            pl.when(cond)(fn)

    def send(src, dst, sid, rid, dev, cond=None):
        c = pltpu.make_async_remote_copy(
            src_ref=src, dst_ref=dst, send_sem=ss.at[sid], recv_sem=rs.at[rid],
            device_id=dev, device_id_type=MESH,
        )
        when(cond, c.start)
        pending.append((c, cond))

    def arrive(dst, rid, cond=None):
        c = pltpu.make_async_remote_copy(
            src_ref=dst, dst_ref=dst, send_sem=ss.at[0], recv_sem=rs.at[rid],
            device_id=pt, device_id_type=MESH,
        )
        when(cond, c.wait_recv)

    def place(fb, rh):
        return pl.multiple_of((fb // n.per_half) * n.half + rh * (n.half // 2) + (fb % n.per_half) * B, B)

    def dot(a, b):
        return jnp.dot(a, b, preferred_element_type=f32)

    def conv(v, w0, w1, w2):
        at = lax.broadcasted_iota(jnp.int32, v.shape, 0)
        one = jnp.where(at >= 1, pltpu.roll(v, 1, axis=0), 0.0)
        two = jnp.where(at >= 2, pltpu.roll(v, 2, axis=0), 0.0)
        return w0 * two + w1 * one + w2 * v

    loads = []

    def load(src, dst):
        c = pltpu.make_async_copy(src, dst, lsem.at[len(loads)])
        c.start()
        loads.append(c)
        return c

    load_tok = load(tok_h, tok)
    load_m = []
    for m, w in enumerate((ow, iw, vw)):
        for h in range(2):
            load_m.append(load(w.at[:, h * CH:(h + 1) * CH], st_m.at[m, h]))
    load_m.append(load(pw, st_p))
    load_f = [load(gw, st_g), load(uw, st_u), load(dn, st_d)]

    barrier = pltpu.get_barrier_semaphore()
    for k in range(1, n.fs):
        pl.semaphore_signal(barrier, inc=1, device_id=(r, (f + k) % n.fs, t), device_id_type=MESH)
    pl.semaphore_signal(barrier, inc=1, device_id=px, device_id_type=MESH)
    pl.semaphore_signal(barrier, inc=1, device_id=pt, device_id_type=MESH)

    for c in load_m:
        c.wait()
    for rh in range(2):
        here = slice(rh * B, (rh + 1) * B)
        for m in range(3):
            ms[here, m * CH:(m + 1) * CH] = st_m[m, 1 - y, here, :].astype(low)
            mw[pl.ds(place(f, rh), B), m * CH:(m + 1) * CH] = st_m[m, y, here, :].astype(low)
        for h, ref, rows in ((1 - y, ms, here), (y, mw, pl.ds(place(f, rh), B))):
            ref[rows, 3 * CH:] = st_p[pl.ds(pl.multiple_of(h * CH + rh * B, B), B), :].astype(low)

    pk[...] = jnp.zeros_like(pk)
    for at, ref in zip(n.slots, (s_o, s_i, s_v, s_g, s_u, s_p, s_d)):
        pk[:, at:at + ref.shape[0]] = ref[...][None, :]
    for q in range(zn):
        @pl.when(z == q)
        def _():
            base = q * Q // LANES * LANES
            for ref, rows in ((channel_taps, slice(0, 3)), (channel_bias, slice(3, 4))):
                taps = ref[:, base:base + n.padded] if len(ref.shape) == 2 else ref[base:base + n.padded][None, :]
                ct[rows, :] = pltpu.roll(taps, n.padded - LANES // 2, axis=1) if q * Q % LANES else taps

    load_tok.wait()

    def square_sum(values):
        return jnp.sum(values * values, axis=1, keepdims=True)

    sq_id = ids(2)

    def share_squares(which, total):
        sq[which] = jnp.broadcast_to(total, (n.rows, LANES))
        send(sq.at[which], sqr.at[which], sq_id + which, sq_id + which, pt)

    own_squares = square_sum(tok[...].astype(f32))
    pl.semaphore_wait(barrier, n.fs + 1)
    share_squares(0, own_squares)

    m1 = ids(2)

    def block_at(fb, rh):
        return mw.at[pl.ds(place(fb, rh), B)]

    def send_m1(rh):
        send(ms.at[pl.ds(pl.multiple_of(rh * B, B), B)], block_at(f, rh), m1 + rh, m1 + rh, py)

    def arrive_m1(rh):
        arrive(block_at(fy, rh), m1 + rh)

    send_m1(r)

    class Line:
        def __init__(self, block):
            self.block = block
            self.up, self.down, self.below, self.above = ids(zn), ids(zn), ids(zn), ids(zn)

        def forward(self, at, k, upward, cond):
            b = self.block(at)
            send(b, b, (self.up if upward else self.down) + k, (self.below if upward else self.above) + k + 1,
                 up if upward else down, cond)

        def start(self):
            self.forward(z, 0, True, can_up)
            self.forward(z, 0, False, can_down)

        def step(self, k, then):
            a, b = (z + zn - k) % zn, (z + k) % zn
            for at, base, upward, cond, more in (
                (a, self.below, True, z >= k, can_up), (b, self.above, False, z < zn - k, can_down),
            ):
                arrive(self.block(at), base + k, cond)
                if k < zn - 1:
                    self.forward(at, k, upward, cond & more)
                then(at, k, upward, cond)

    own_line = Line(lambda at: block_at(2 * at + y, r))
    other_line = Line(lambda at: block_at(2 * at + 1 - y, r))
    own_line.start()

    def inverse_norm_of(which, own):
        arrive(sqr.at[which], sq_id + which)
        return lax.rsqrt((own + sqr[which][:, :1]) / n.features + epsilon)

    def normalize(values, rows, inverse, gain, dst):
        for fl in range(n.per_half):
            for rh in range(2):
                here = slice((2 * fl + rh) * B, (2 * fl + rh + 1) * B)
                there = slice((rh * n.per_half + fl) * B, (rh * n.per_half + fl + 1) * B)
                dst[rows, there] = (values[rows, here].astype(f32) * inverse[rows] * gain[:, here]).astype(low)

    whole = slice(0, n.rows)
    parts = [slice(c * n.rows // 2, (c + 1) * n.rows // 2) for c in range(2)]

    normalize(tok, whole, inverse_norm_of(0, own_squares), mg, xg.at[y, t])
    x_y, x_t = ids(), ids(2)
    send(xg.at[y, t], xg.at[y, t], x_y, x_y, py)
    send(xg.at[y, t], xg.at[y, t], x_t, x_t, pt)
    send_m1(1 - r)

    scale_s, scale_r = ids(n.fs), ids(n.fs)
    sc[f] = pk[...]
    for k in range(1, n.fs):
        send(pk, sc.at[f], scale_s + k, scale_r + f, (r, (f + k) % n.fs, t))

    mx = ids(4 * zn)

    def over_x(which, blk):
        def then(at, k, upward, cond):
            s = mx + 4 * k + 2 * which + (1 if upward else 0)
            send(blk(at), blk(at), s, s, px, cond)
        return then

    for c in load_f:
        c.wait()

    def tiles(rows, q):
        base = q * Q // LANES * LANES
        g = st_g[rows, base:base + n.padded]
        u = st_u[rows, base:base + n.padded]
        if q * Q % LANES:
            g = pltpu.roll(g, n.padded - LANES // 2, axis=1)
            u = pltpu.roll(u, n.padded - LANES // 2, axis=1)
        parts = []
        for j in range(n.full):
            parts += [g[:, j * LANES:(j + 1) * LANES], u[:, j * LANES:(j + 1) * LANES]]
        lane = lax.broadcasted_iota(jnp.int32, (B, LANES), 1)
        parts.append(jnp.where(lane < LANES // 2, g[:, n.full * LANES:], pltpu.roll(u[:, n.full * LANES:], LANES // 2, axis=1)))
        return parts

    for q in range(zn):
        @pl.when(z == q)
        def _():
            for rh in range(2):
                for j, piece in enumerate(tiles(pl.ds(rh * B, B), q)):
                    gu[pl.ds(place(f, rh), B), j * LANES:(j + 1) * LANES] = piece.astype(low)

        @pl.when(z != q)
        def _():
            for j, piece in enumerate(tiles(pl.ds(pl.multiple_of(r * B, B), B), q)):
                sg[q, :, j * LANES:(j + 1) * LANES] = piece.astype(low)

        sd[q] = st_d[pl.ds(pl.multiple_of(q * Q + r * (Q // 2), 16), Q // 2), :].astype(low)
    dw[f] = st_d[pl.ds(pl.multiple_of(z * Q, 16), Q), :].astype(low)

    def gu_at(fb, rh):
        return gu.at[pl.ds(place(fb, rh), B)]

    def dw_at(fb, rh):
        return dw.at[fb, pl.ds(pl.multiple_of(rh * (Q // 2), 16), Q // 2)]

    fy_own = ids(4)
    for rh in range(2):
        send(gu_at(f, rh), gu_at(f, rh), fy_own + rh, fy_own + rh, py)
    send(dw_at(f, r), dw_at(f, r), fy_own + 2, fy_own + 2, py)

    f1, f2y, f2x, f2d = ids(2 * zn), ids(2 * zn), ids(2 * zn), ids(2 * zn)

    def across(k):
        if k == 1:
            return z + 1 - 2 * (z % 2)
        if k == 2:
            return z + 2 - 4 * (z // 2)
        return zn - 1 - z

    def stage_one(k, cond):
        q = across(k)
        dev = (r, 2 * q + y, t)
        send(sg.at[q], gu_at(f, r), f1 + 2 * k, f1 + 2 * k, dev, cond)
        send(sd.at[q], dw_at(f, r), f1 + 2 * k + 1, f1 + 2 * k + 1, dev, cond)

    def held(k):
        fb = 2 * across(k) + y
        return enumerate((gu_at(fb, r), dw_at(fb, r)))

    def pieces_over_x(k, cond):
        for i, ref in held(k):
            arrive(ref, f1 + 2 * k + i, cond)
            send(ref, ref, f2x + 2 * k + i, f2x + 2 * k + i, px, cond)

    def pieces_over_y(k):
        for i, ref in held(k):
            send(ref, ref, f2y + 2 * k + i, f2y + 2 * k + i, py)

    def over_y(k, i):
        return k + i == zn - 1

    def refs_of(k, own_y, rh):
        fb = 2 * across(k) + (y if own_y else 1 - y)
        return gu_at(fb, rh), dw_at(fb, rh)

    def pieces_on(k):
        for i in range(2):
            if over_y(k, i):
                ref, base, dev = refs_of(k, True, 1 - r)[i], f2x, py
            else:
                ref, base, dev = refs_of(k, False, r)[i], f2y, px
            arrive(ref, base + 2 * k + i)
            send(ref, ref, f2d + 2 * k + i, f2d + 2 * k + i, dev)

    def pieces_end(k, i):
        if over_y(k, i):
            arrive(refs_of(k, False, r)[i], f2y + 2 * k + i)
        else:
            arrive(refs_of(k, True, 1 - r)[i], f2x + 2 * k + i)
        arrive(refs_of(k, False, 1 - r)[i], f2d + 2 * k + i)

    arrive_m1(r)
    other_line.start()
    stage_one(1, ends)
    own_x, other_x = over_x(0, own_line.block), over_x(1, other_line.block)
    own_line.step(1, own_x)
    other_line.step(1, other_x)
    own_line.step(2, own_x)
    arrive(xg.at[1 - y, t], x_y)
    send(xg.at[1 - y, t], xg.at[1 - y, t], x_t + 1, x_t + 1, pt)
    other_line.step(2, other_x)
    stage_one(2, ends)
    stage_one(3, inner)
    own_line.step(3, own_x)
    other_line.step(3, other_x)

    for k in range(1, n.fs):
        fk = (f + k) % n.fs
        arrive(sc.at[fk], scale_r + fk)
    for m, at in enumerate(n.slots[:3]):
        slot = slice(at, at + LANES)
        for j in range(CH // LANES):
            fb = n.per_half * y + 2 * j
            msc[m:m + 1, j * LANES:(j + 1) * LANES] = sc[fb][:, slot] + pltpu.roll(sc[fb + 1][:, slot], LANES // 2, axis=1)
    for i, at in enumerate(n.slots[3:5]):
        first, second = (
            jnp.concatenate([sc[2 * z + h][:, at:at + n.padded // 2], jnp.zeros((1, n.padded // 2), f32)], axis=1)
            for h in range(2)
        )
        gsus[i:i + 1, :] = first + pltpu.roll(second, Q // 2, axis=1)
    arrive_m1(1 - r)
    for i in range(2):
        arrive(xg.at[y if i == 0 else 1 - y, 1 - t], x_t + i)
    near = z // 2

    def arrive_mixer(k, own_half, streams=(0, 1)):
        for side, at, cond in ((1, (z + zn - k) % zn, z >= k), (0, (z + k) % zn, z < zn - k)):
            for which in streams:
                fb = 2 * at + (1 - y if which else y)
                same = at // 2 == near
                arrive(block_at(fb, 1 - r), mx + 4 * k + 2 * which + side, cond & (same if own_half else ~same))

    arrive_mixer(1, True)
    near_rows = pl.ds(pl.multiple_of(near * n.half, n.half), n.half)
    far_rows = pl.ds(pl.multiple_of((1 - near) * n.half, n.half), n.half)
    for i, sy in enumerate((1 - y, y)):
        for m in range(3):
            here = slice(m * CH, (m + 1) * CH)
            acc[2 + i, :, here] = dot(xg[sy, near], mw[near_rows, here])
    arrive_mixer(1, False)
    stage_one(1, inner)
    arrive_mixer(2, False)
    arrive_mixer(3, False)

    y_lanes = pl.ds(pl.multiple_of(y * CH, CH), CH)
    m_taps = [mt[k:k + 1, y_lanes] for k in range(3)]
    mt_id, my_id = ids(3), ids(2)
    pad = 16

    def wide(fl):
        return slice(fl * D, (fl + 1) * D)

    def with_past(rows):
        first = max(rows.start - pad, 0)
        return slice(first, rows.stop), rows.start - first

    def mix(i, rows, at):
        sy = (1 - y, y)[i]
        long, drop = with_past(rows)

        def part(m):
            here = slice(m * CH, (m + 1) * CH)
            return (acc[2 + i, long, here] + dot(xg[sy, 1 - near, long], mw[far_rows, here])) * msc[m:m + 1, :]

        cv = conv(part(1) * part(2), *m_taps)
        mixed = (part(0) * cv).astype(low)[drop:]

        def project(fb):
            return dot(mixed, jnp.concatenate([mw[pl.ds(place(fb, rh), B), 3 * CH:] for rh in range(2)], axis=0))

        for fl in range(n.per_half):
            mps[i, rows, wide(fl)] = project(n.per_half * (1 - t) + fl).astype(low)
        send(mps.at[i, rows], mpr.at[i, rows], mt_id + at, mt_id + at, pt)
        for fl in range(n.per_half):
            acc[i, rows, wide(fl)] = project(n.per_half * t + fl)

    for c, rows in enumerate(parts):
        if c == 1:
            pieces_over_x(1, ends)
        mix(0, rows, c)
        arrive(mpr.at[0, rows], mt_id + c)
        ys[rows] = (acc[0, rows] + mpr[0, rows].astype(f32)).astype(low)
        send(ys.at[rows], yr.at[rows], my_id + c, my_id + c, py)
    stage_one(2, inner)
    arrive(dw_at(fy, r), fy_own + 2)
    send(dw_at(fy, r), dw_at(fy, r), fy_own + 3, fy_own + 3, px)
    pieces_over_x(1, inner)
    mix(1, whole, 2)
    arrive(mpr.at[1], mt_id + 2)

    pieces_over_x(3, inner)
    pieces_over_x(2, inner)

    pieces_over_y(1)
    arrive(yr.at[parts[0]], my_id)
    stage_one(3, ends)
    arrive(yr.at[parts[1]], my_id + 1)
    pieces_over_x(2, ends)
    total_sq = None
    for fl in range(n.per_half):
        w = wide(fl)
        added = (acc[1, :, w] + mpr[1, :, w].astype(f32) + yr[:, w].astype(f32)) * sc[n.per_half * t + fl][:, n.slots[5]:n.slots[5] + D]
        middle = (tok[:, w].astype(f32) + added).astype(low)
        mid[:, w] = middle
        part_sq = square_sum(middle.astype(f32))
        total_sq = part_sq if total_sq is None else total_sq + part_sq
    share_squares(1, total_sq)
    inverse = inverse_norm_of(1, total_sq)

    n_t = ids(4 * zn)
    token_lines = []
    for c, rows in enumerate(parts):
        normalize(mid, rows, inverse, cg, ng.at[z, t])
        line = Line(lambda at, rows=rows: ng.at[at, t, rows])
        line.start()
        token_lines.append(line)
        send(line.block(z), line.block(z), n_t + c, n_t + c, pt)

    def token_step(k):
        for c, line in enumerate(token_lines):
            def to_core(at, k, upward, cond):
                s = n_t + 4 * k + (2 if upward else 0) + c
                send(line.block(at), line.block(at), s, s, pt, cond)

            line.step(k, to_core)

    pieces_over_y(2)
    pieces_over_x(3, ends)
    pieces_over_y(3)
    pieces_on(1)
    token_step(1)
    pieces_on(2)
    pieces_on(3)
    token_step(2)
    def core_step(k):
        for c, rows in enumerate(parts):
            for side, at, cond in ((2, (z + zn - k) % zn, z >= k), (0, (z + k) % zn, z < zn - k)):
                arrive(ng.at[at, 1 - t, rows], n_t + 4 * k + side + c, cond)

    for c, rows in enumerate(parts):
        arrive(ng.at[z, 1 - t, rows], n_t + c)
    core_step(1)
    core_step(2)
    for rh in range(2):
        arrive(gu_at(fy, rh), fy_own + rh)
    for k in range(1, zn):
        pieces_end(k, 0)

    p_t, z_s, z_b, z_a = ids(6), ids(2 * zn), ids(2 * zn), ids(2 * zn)
    side = z // 2
    order = (2 - side, 3 * (1 - side), z + 1 - 2 * (z % 2), z)

    def to_line(i, c, cond_up, cond_down):
        s, here = order[i], parts[c]
        for dst, base, dev, cond in ((zb, z_b, up, cond_up), (za, z_a, down, cond_down)):
            send(zs.at[s, here], dst.at[s, here], z_s + 2 * i + c, base + 2 * s + c, dev, cond)

    def chain(i, c):
        s, here = order[i], parts[c]
        for ref, base, cond in ((zb, z_b, inner & (s > z)), (za, z_a, inner & (s < z))):
            arrive(ref.at[s, here], base + 2 * s + c, cond)

            @pl.when(cond)
            def _():
                zs[s, here] = (acc[i, here] + ref[s, here].astype(f32)).astype(low)

        to_line(i, c, inner & (s > z), inner & (s < z))

    def gated(a, here):
        c = conv(a * gsus[0:1, here], ct[0:1, here], ct[1:2, here], ct[2:3, here]) + ct[3:4, here]
        return c / (1.0 + jnp.exp(-c))

    def hidden(s, rows):
        long, drop = with_past(rows)

        def product(at, width):
            here = slice(at, at + width)
            return dot(ng[s, 0, long], gu[:n.half, here]) + dot(ng[s, 1, long], gu[n.half:, here])

        for j in range(n.full):
            a = product(j * 2 * LANES, 2 * LANES)
            here = slice(j * LANES, (j + 1) * LANES)
            hid[rows, here] = (gated(a[:, :LANES], here) * (a[:, LANES:] * gsus[1:2, here])).astype(low)[drop:]
        a = product(n.full * 2 * LANES, LANES)
        here = slice(n.full * LANES, n.padded)
        last = gated(a, here) * (pltpu.roll(a, LANES // 2, axis=1) * gsus[1:2, here])
        hid[rows, n.full * LANES:] = last.astype(low)[drop:, :n.tail]

    def back(i, rows, at):
        hid_v = hid[rows]
        for fl in range(n.per_half):
            ps[i, rows, wide(fl)] = dot(hid_v, dw[n.per_half * (1 - t) + fl]).astype(low)
        send(ps.at[i, rows], pr.at[i, rows], p_t + at, p_t + at, pt)
        for fl in range(n.per_half):
            acc[i, rows, wide(fl)] = dot(hid_v, dw[n.per_half * t + fl])
        arrive(pr.at[i, rows], p_t + at)
        acc[i, rows] = acc[i, rows] + pr[i, rows].astype(f32)
        if i < zn - 1:
            @pl.when(ends)
            def _():
                zs[order[i], rows] = acc[i, rows].astype(low)

    def outward(i, c):
        to_line(i, c, z == 0, z == zn - 1)

    hidden(order[0], parts[0])
    arrive(dw_at(fy, 1 - r), fy_own + 3)
    for k in range(1, zn):
        pieces_end(k, 1)
    back(0, parts[0], 0)
    outward(0, 0)
    hidden(order[0], parts[1])
    back(0, parts[1], 1)
    token_step(3)
    core_step(3)
    for c in range(2):
        hidden(order[1], parts[c])
        back(1, parts[c], 2 + c)
        outward(1, c)
    outward(0, 1)
    hidden(order[2], whole)
    back(2, whole, 4)
    outward(2, 0)
    outward(2, 1)
    chain(0, 0)
    chain(1, 0)
    hidden(order[3], whole)
    back(3, whole, 5)
    for i, c in ((1, 1), (2, 0), (0, 1), (2, 1)):
        chain(i, c)

    for c, here in enumerate(parts):
        for ref, base, cond in ((zb, z_b, can_down), (za, z_a, can_up)):
            arrive(ref.at[z, here], base + 2 * z + c, cond)

            @pl.when(cond)
            def _():
                acc[zn - 1, here] = acc[zn - 1, here] + ref[z, here].astype(f32)

    for fl in range(n.per_half):
        w = wide(fl)
        scaled = acc[zn - 1, :, w] * sc[n.per_half * t + fl][:, n.slots[6]:n.slots[6] + D]
        out[:, w] = (mid[:, w].astype(f32) + scaled).astype(low)

    for c, cond in pending:
        when(cond, c.wait_send)
    assert used[0] <= SEMAPHORES, used[0]


def in_one_kernel(
    n, tokens, mixer_gain, outer_weight, inner_weight, value_weight, outer_scale, inner_scale,
    value_scale, mixer_taps, mixer_project, project_scale, channel_gain, gate_weight, gate_scale,
    up_weight, up_scale, channel_taps, channel_bias, down_weight, down_scale,
):
    f32, zn = jnp.float32, GROUPS
    scales = (outer_scale, inner_scale, value_scale, gate_scale, up_scale, project_scale, down_scale)
    vm, anywhere = pl.BlockSpec(memory_space=pltpu.VMEM), pl.BlockSpec(memory_space=pl.ANY)
    rows, half, features = n.rows, n.half, n.features

    def V(shape, dtype=low):
        return pltpu.VMEM(shape, dtype)

    scratch = [
        V((rows, half)),
        V((3, 2, n.depth, n.chan), f32), V((n.cols, n.depth), f32),
        V((n.depth, zn * n.quarter), f32), V((n.depth, zn * n.quarter), f32), V((zn * n.quarter, n.depth), f32),
        V((features, 3 * n.chan + n.depth)), V((n.depth, 3 * n.chan + n.depth)),
        V((features, n.wide)), V((n.fs, n.quarter, n.depth)),
        V((zn, n.block, n.wide)), V((zn, n.quarter // 2, n.depth)),
        V((1, n.slots[-1]), f32), V((n.fs, 1, n.slots[-1]), f32), V((3, n.chan), f32), V((2, n.padded), f32), V((4, n.padded), f32),
        V((2, rows, LANES), f32), V((2, rows, LANES), f32),
        V((2, 2, rows, half)), V((2, rows, half)), V((2, rows, half)), V((rows, half)), V((rows, half)),
        V((rows, half)), V((zn, 2, rows, half)), V((rows, n.quarter)), V((zn, rows, half), f32),
        V((zn, rows, half)), V((zn, rows, half)), V((zn, rows, half)), V((zn, rows, half)), V((zn, rows, half)),
        pltpu.SemaphoreType.DMA((16,)), pltpu.SemaphoreType.DMA((SEMAPHORES,)), pltpu.SemaphoreType.DMA((SEMAPHORES,)),
    ]
    return pl.pallas_call(
        functools.partial(layer_kernel, n),
        out_shape=jax.ShapeDtypeStruct(tokens.shape, tokens.dtype),
        in_specs=[anywhere] + [vm] * 12 + [anywhere] * 7,
        out_specs=vm,
        scratch_shapes=scratch,
        compiler_params=pltpu.CompilerParams(
            collective_id=0, has_side_effects=True, vmem_limit_bytes=VMEM_BYTES
        ),
    )(
        tokens, mixer_gain[None, :], channel_gain[None, :], mixer_taps, channel_taps, channel_bias, *scales,
        outer_weight, inner_weight, value_weight, mixer_project, gate_weight, up_weight, down_weight,
    )


def solution(mesh):
    placed = (
        P(("rep", "fs"), "tp"),
        P("tp"),
        P("fs", "tp"),
        P("fs", "tp"),
        P("fs", "tp"),
        P(("tp", "fs")),
        P(("tp", "fs")),
        P(("tp", "fs")),
        P(None, "tp"),
        P("tp", "fs"),
        P("fs"),
        P("tp"),
        P("fs", "tp"),
        P(("tp", "fs")),
        P("fs", "tp"),
        P(("tp", "fs")),
        P(None, "tp"),
        P("tp"),
        P("tp", "fs"),
        P("fs"),
    )
    return jax.shard_map(
        per_device, mesh=mesh, in_specs=placed, out_specs=P(("rep", "fs"), "tp"), check_vma=False
    )
```
